32 devices in a mesh: ep: 8 (over z, x), tp: 4 (over y, core).
Axes of the slice: x: 2, y: 2, z: 4, core: 2. Of those that a mesh axis runs over, the one named last changes fastest.
Arguments:
- tokens: bfloat16 [1024, 4096], P('ep', 'tp'), may hold values from -16 to 16
- expert_ids: int32 [1024, 2], P('ep'), may hold values from 0 to 7, as said below
- group_weight: float32 [1024], P('ep'), may hold values from 0.25 to 1
- expert_weight: float32 [1024, 2], P('ep'), may hold values from 0.1 to 1
- w_gate: bfloat16 [8, 4096, 512], P('ep', None, 'tp'), may hold values from -0.09375 to 0.09375
- w_up: bfloat16 [8, 4096, 512], P('ep', None, 'tp'), may hold values from -0.09375 to 0.09375
- w_down: bfloat16 [8, 512, 4096], P('ep', None, 'tp'), may hold values from -0.5 to 0.5
- norm_gain: float32 [4096], P('tp'), may hold values from 0.1 to 1.9
- norm_bias: float32 [4096], P('tp'), may hold values from -3 to 3
Outputs:
- normed: bfloat16 [1024, 4096], P('ep', 'tp')
The draws below stay inside these ranges and needn't reach their ends.
Inputs may be any that keep to these rules, and one draw needn't show every extreme that they name: `expert_ids`: each row names 2 different experts of one group, a group being 2 consecutive ids; in the rows of one ep index each group is named by a 4-th of the rows. In the rows of one ep index no expert is named more than 32 times, and in every group one expert is named exactly 32 times in the rows of every ep index.
All inputs are finite; a program needn't handle non-finite values.
Results may differ from the reference program's by a relative error of at most 0.0045.
Values may be sent and summed in bfloat16 or wider, within the bound.
A program may use at most 64 MiB of HBM per device.

```python
import math
import jax
import jax.numpy as jnp
from jax import lax

D = 4096
FF = 512
GROUPS = 4
TOP_K = 2
TOK_DEV = 128
EXPERTS = 8
CAP = 32
TOKENS = 1024
N_EP = 8


def draw_tokens(key, part):
    quarter = (jnp.arange(D, dtype=jnp.int32) // (D // 4)).astype(jnp.float32)
    column_scale = 0.5 + 0.5 * quarter
    column_shift = 0.6 * (quarter - 1.5)
    values = jax.random.normal(jax.random.fold_in(key, 5), (TOKENS, D), jnp.float32)
    values = jnp.clip(values * column_scale[None, :] + column_shift[None, :], -16.0, 16.0)
    return values.astype(jnp.bfloat16)


def draw_expert_ids(key, part):
    per_group = EXPERTS // GROUPS
    pair_count = TOK_DEV // GROUPS
    block_count = TOKENS // TOK_DEV
    fixed_local = jax.random.randint(jax.random.fold_in(key, 1), (GROUPS,), 0, per_group)
    local_ids = jnp.arange(per_group, dtype=jnp.int32)
    pair_index = jnp.arange(pair_count, dtype=jnp.int32)
    first_rank = pair_index // CAP
    second_rank = (pair_index + pair_count) // CAP

    def one_block(index):
        block_key = jax.random.fold_in(key, index + 7)
        scores = jax.random.randint(jax.random.fold_in(block_key, 0), (GROUPS, per_group), 0, 1 << 20)
        scores = scores * per_group + local_ids[None, :]
        scores = jnp.where(local_ids[None, :] == fixed_local[:, None], -1, scores)
        order = jnp.argsort(scores, axis=1, stable=True).astype(jnp.int32)
        first = order[:, first_rank]
        second = order[:, second_rank]
        local_pair = jnp.stack([first, second], axis=-1)
        global_pair = local_pair + (jnp.arange(GROUPS, dtype=jnp.int32) * per_group)[:, None, None]
        flat_pairs = global_pair.reshape(TOK_DEV, 2)
        shuffle = jax.random.permutation(jax.random.fold_in(block_key, 1), TOK_DEV)
        return flat_pairs[shuffle]
    drawn = jax.vmap(one_block)(jnp.arange(block_count, dtype=jnp.int32))
    return drawn.reshape(TOKENS, 2).astype(jnp.int32)


def level_of(rng, extent, pieces, low, largest):
    factor_of, own = 1.0, jax.random.fold_in(rng, 6)
    for dim, shards_of in pieces:
        draws = jnp.exp(jax.random.uniform(jax.random.fold_in(own, dim), (shards_of,), jnp.float32, low / len(pieces), largest / len(pieces)))
        factor_of = factor_of * jnp.repeat(draws, extent[dim] // shards_of).reshape([-1 if axis == dim else 1 for axis in range(len(extent))])
    return factor_of


def noise(stream_key, shape, scale, reach, split=(), kind=jnp.bfloat16):
    gain = level_of(stream_key, shape, split, -0.22, 0.18) if split else 1.0
    values = jax.random.normal(stream_key, shape, jnp.float32) * scale * gain
    return jnp.minimum(jnp.maximum(values, -reach), reach).astype(kind)


def setup_inputs(seed: int = 0) -> dict:
    key_of = jax.random.split(jax.random.key(seed), 10)
    return {
        "tokens": draw_tokens(jax.random.fold_in(key_of[9], 71), 0),
        "expert_ids": draw_expert_ids(jax.random.fold_in(key_of[9], 71), 0),
        "group_weight": jnp.clip(jnp.exp(math.log(1.0) - 1.3862944 * jax.random.uniform(key_of[2], (TOKENS,), jnp.float32) ** level_of(key_of[2], (TOKENS,), ((0, 8),), -0.2, 0.2)), 0.25, 1.0),
        "expert_weight": jnp.clip(jnp.exp(math.log(1.0) - 2.3025851 * jax.random.uniform(key_of[3], (TOKENS, TOP_K), jnp.float32) ** level_of(key_of[3], (TOKENS, TOP_K), ((0, 8),), -0.2, 0.2)), 0.1, 1.0),
        "w_gate": noise(key_of[4], (EXPERTS, D, FF), D ** -0.5, 0.09375, ((0, 8), (2, 4))),
        "w_up": noise(key_of[5], (EXPERTS, D, FF), D ** -0.5, 0.09375, ((0, 8), (2, 4))),
        "w_down": noise(key_of[6], (EXPERTS, FF, D), (FF // 4) ** -0.5, 0.5, ((0, 8), (2, 4))),
        "norm_gain": jnp.clip(1.0 + 0.18 * jax.random.normal(key_of[7], (D,), jnp.float32), 0.1, 1.9),
        "norm_bias": noise(key_of[8], (D,), 0.5, 3.0, ((0, 4),), jnp.float32),
    }


residual_scale = 2.0 ** 0.5
norm_eps = 1e-05

def reference(tokens, expert_ids, group_weight, expert_weight, w_gate, w_up, w_down, norm_gain, norm_bias):
    block_count = TOKENS // TOK_DEV
    rows_per = N_EP * CAP
    flat_ids = expert_ids.reshape(block_count, TOK_DEV * TOP_K).astype(jnp.int32)
    one_hot = (flat_ids[:, :, None] == jnp.arange(EXPERTS, dtype=jnp.int32)[None, None, :]).astype(jnp.int32)
    prior_counts = jnp.cumsum(one_hot, axis=1) - one_hot
    slot_index = lax.optimization_barrier(jnp.sum(prior_counts * one_hot, axis=2)).astype(jnp.int32)
    block_start = (jnp.arange(block_count, dtype=jnp.int32) * CAP)[:, None]
    position = (flat_ids * rows_per + block_start + slot_index).reshape(-1).astype(jnp.int32)
    owner_token = (jnp.arange(TOKENS * TOP_K, dtype=jnp.int32) // TOP_K).astype(jnp.int32)
    slot_table = jnp.full((EXPERTS * rows_per,), TOKENS, jnp.int32).at[position].set(owner_token)
    padded = jnp.concatenate([tokens, jnp.zeros((1, D), tokens.dtype)], axis=0)

    def expert(inputs):
        table_rows, gate_w, up_w, down_w = inputs
        row_block = padded[table_rows]
        gate_sum = jnp.dot(row_block, gate_w, preferred_element_type=jnp.float32)
        up_sum = jnp.dot(row_block, up_w, preferred_element_type=jnp.float32)
        hidden = (jax.nn.silu(gate_sum) * up_sum).astype(jnp.bfloat16)
        return jnp.dot(hidden, down_w, preferred_element_type=jnp.float32).astype(jnp.bfloat16)
    results = lax.map(expert, (slot_table.reshape(EXPERTS, rows_per), w_gate, w_up, w_down))
    picked = results.reshape(EXPERTS * rows_per, D)[position].reshape(TOKENS, TOP_K, D).astype(jnp.float32)
    share_weight = group_weight[:, None] * expert_weight / lax.optimization_barrier(jnp.sum(expert_weight, axis=1, keepdims=True))
    routed = jnp.einsum('tk,tkd->td', share_weight.astype(jnp.float32), picked)
    mixed = residual_scale * tokens.astype(jnp.float32) + routed
    center = lax.optimization_barrier(jnp.mean(mixed, axis=1, keepdims=True))
    centered = mixed - center
    spread = lax.optimization_barrier(jnp.mean(centered * centered, axis=1, keepdims=True))
    normed = centered * lax.rsqrt(spread + norm_eps) * norm_gain[None, :] + norm_bias[None, :]
    return normed.astype(jnp.bfloat16)
```

```python
import functools

import jax
import jax.numpy as jnp
from jax import lax
from jax.experimental import pallas as pl
from jax.experimental.pallas import tpu as pltpu
from jax.sharding import PartitionSpec as P

D = 4096
GROUPS = 4
TOP_K = 2


residual_scale = 2.0**0.5
norm_eps = 1e-05


def on_device(
    tokens, expert_ids, group_weight, expert_weight, w_gate, w_up, w_down, norm_gain, norm_bias
):
    tok_count = tokens.shape[0]
    expert_count = lax.axis_size("ep")
    capacity = min(tok_count // GROUPS, 3 * TOP_K * tok_count // (2 * expert_count))
    pair_count = tok_count * TOP_K
    flat_ids = expert_ids.reshape(pair_count)
    one_hot = (flat_ids[:, None] == jnp.arange(expert_count, dtype=jnp.int32)[None, :]).astype(
        jnp.float32
    )
    earlier = (jnp.arange(pair_count)[:, None] > jnp.arange(pair_count)[None, :]).astype(
        jnp.float32
    )
    prior_counts = jnp.dot(
        earlier, one_hot, preferred_element_type=jnp.float32, precision=lax.Precision.HIGHEST
    )
    slot_index = jnp.sum(prior_counts * one_hot, axis=1).astype(jnp.int32)
    position = flat_ids * capacity + slot_index
    owner_token = jnp.arange(pair_count, dtype=jnp.int32) // TOP_K
    slot_table = (
        jnp.full((expert_count * capacity,), tok_count, jnp.int32).at[position].set(owner_token)
    )
    gate_local = w_gate[0]
    up_local = w_up[0]
    down_local = w_down[0]
    padded = jnp.concatenate([tokens, jnp.zeros((1, tokens.shape[1]), tokens.dtype)], axis=0)
    outgoing = padded[slot_table].reshape(expert_count, capacity, tokens.shape[1])
    arrived = lax.all_to_all(outgoing, "ep", split_axis=0, concat_axis=0, tiled=True)
    sources, slot_count, slice_width = arrived.shape
    row_block = arrived.reshape(sources * slot_count, slice_width)
    row_piece = lax.all_gather(row_block, "tp", axis=1, tiled=True)
    gate_sum = jnp.dot(row_piece, gate_local, preferred_element_type=jnp.float32)
    up_sum = jnp.dot(row_piece, up_local, preferred_element_type=jnp.float32)
    hidden = (jax.nn.silu(gate_sum) * up_sum).astype(jnp.bfloat16)
    result = jnp.dot(
        lax.all_gather(hidden, "tp", axis=1, tiled=True),
        down_local,
        preferred_element_type=jnp.float32,
    )
    result = result.astype(jnp.bfloat16).reshape(sources, slot_count, down_local.shape[1])
    returned = lax.all_to_all(result, "ep", split_axis=0, concat_axis=0, tiled=True)
    flat_rows = returned.reshape(expert_count * capacity, returned.shape[2])
    picked = flat_rows[position].reshape(tok_count, TOP_K, returned.shape[2]).astype(jnp.float32)
    share_weight = (
        group_weight[:, None] * expert_weight / jnp.sum(expert_weight, axis=1, keepdims=True)
    )
    routed = jnp.einsum("tk,tkd->td", share_weight, picked)
    mixed = residual_scale * tokens.astype(jnp.float32) + routed
    first_sum, second_sum = lax.psum((jnp.sum(mixed, axis=1), jnp.sum(mixed * mixed, axis=1)), "tp")
    center = first_sum / D
    spread = second_sum / D - center * center
    centered = mixed - center[:, None]
    normed = (
        centered * lax.rsqrt(spread + norm_eps)[:, None] * norm_gain[None, :] + norm_bias[None, :]
    )
    return normed.astype(jnp.bfloat16)


MESH = pl.DeviceIdType.MESH
F32 = jnp.float32
BF16 = jnp.bfloat16
(TO_PLANE, TO_PLANE_2, SHARES, CORE_OWN, ACROSS_X, ACROSS_Y, CORE_X, CORE_Y, RELAY_X, RELAY_Y,
 CORE_RX, CORE_RY, HIDDEN, RESULT, RESULT_2, BACK, BACK_2, ACROSS_X2, ACROSS_Y2) = range(19)
KINDS = 19


def flip(value, bits):
    bit = 1
    while bit <= bits:
        if bits & bit:
            value = value + bit - 2 * bit * lax.rem(lax.div(value, bit), 2)
        bit *= 2
    return value


def layer_kernel(
    n_plane, n_tp,
    tokens_hbm, ids_hbm, group_hbm, expert_hbm, gate_hbm, up_hbm, down_hbm, gain_hbm, bias_hbm,
    normed_out,
    tokens_ref, ids_ref, group_ref, expert_ref, gain_ref, bias_ref,
    w_in, w_out, outgoing, share_out, share_in, share_far, rows, hidden, own_part, result_out,
    result_in, back_out, back_in, stats_out, stats_in,
    send_sem, recv_sem, hidden_send, hidden_recv, stats_send, stats_recv, load_sem, entered,
):
    ep = lax.axis_index("ep")
    q = lax.axis_index("tp")
    z, x = lax.div(ep, 2), lax.rem(ep, 2)
    ox = 1 - x
    q_core, q_y, q_diag = flip(q, 1), flip(q, 2), flip(q, 3)
    core_peer, y_peer, diag_peer = (ep, q_core), (ep, q_y), (ep, q_diag)
    x_peer = (z * 2 + ox, q)

    def at_plane(zz):
        return (zz * 2 + x, q)

    last = n_plane - 1
    inside = lax.div(z * (last - z), 2)
    z1 = 1 + lax.rem(z, 2)
    z3 = last * (1 - lax.div(z, 2))
    z2 = 6 - z - z1 - z3
    outer = last * (z - 1) * inside

    tok, width = tokens_ref.shape
    cap = tok // n_plane
    half = cap // 2
    inner = gate_hbm.shape[2]

    inputs = [
        pltpu.make_async_copy(source, target, load_sem.at[3 + i])
        for i, (source, target) in enumerate((
            (ids_hbm, ids_ref), (tokens_hbm, tokens_ref), (group_hbm, group_ref),
            (expert_hbm, expert_ref), (gain_hbm, gain_ref), (bias_hbm, bias_ref),
        ))
    ]
    for load in inputs:
        load.start()

    barrier = pltpu.get_barrier_semaphore()
    for peer in (at_plane(z1), x_peer, core_peer, y_peer, diag_peer):
        pl.semaphore_signal(barrier, inc=1, device_id=peer, device_id_type=MESH)

    @pl.when(inside == 1)
    def _():
        pl.semaphore_signal(barrier, inc=1, device_id=at_plane(outer), device_id_type=MESH)

    loads = [
        pltpu.make_async_copy(gate_hbm.at[0], w_in.at[:, pl.ds(0, inner)], load_sem.at[0]),
        pltpu.make_async_copy(up_hbm.at[0], w_in.at[:, pl.ds(inner, inner)], load_sem.at[1]),
        pltpu.make_async_copy(down_hbm.at[0], w_out, load_sem.at[2]),
    ]
    for load in loads:
        load.start()

    inputs[0].wait()
    first = ids_ref[0:1, :]
    group_row = (first >> 1).astype(F32)
    on_lanes = jnp.broadcast_to(group_row, (tok, tok))
    on_rows = jnp.transpose(on_lanes)
    ii = lax.broadcasted_iota(jnp.int32, (tok, tok), 0)
    jj = lax.broadcasted_iota(jnp.int32, (tok, tok), 1)
    same = on_lanes == on_rows
    zero, one = jnp.zeros((tok, tok), F32), jnp.ones((tok, tok), F32)
    rank_row = jnp.sum(jnp.where(same & (ii < jj), one, zero), axis=0, keepdims=True)
    rank_col = jnp.sum(jnp.where(same & (jj < ii), one, zero), axis=1, keepdims=True)
    place_row = group_row * cap + rank_row
    place_col = on_rows[:, 0:1] * cap + rank_col
    to_slot = jnp.broadcast_to(place_row, (tok, tok)) == ii.astype(F32)
    to_token = jnp.broadcast_to(place_col, (tok, tok)) == jj.astype(F32)

    inputs[1].wait()
    sorted_rows = jnp.dot(
        jnp.where(to_slot, one, zero).astype(BF16), tokens_ref[...], preferred_element_type=F32
    ).astype(BF16)
    outgoing[...] = sorted_rows.reshape(n_plane, cap, width)
    rows[q, x, z] = outgoing[z]

    inputs[2].wait()
    inputs[3].wait()
    weights = expert_ref[...]
    share = group_ref[...] * weights / jnp.sum(weights, axis=0, keepdims=True)
    even = (first & 1) == 0
    for k in range(2):
        chosen = jnp.where(even, share[k:k + 1, :], share[1 - k:2 - k, :])
        by_token = jnp.transpose(jnp.broadcast_to(chosen, (tok, tok)))
        share_out[k:k + 1, :] = jnp.sum(jnp.where(to_token, by_token, zero), axis=0, keepdims=True)
    share_in[z] = share_out[...]

    pl.semaphore_wait(barrier, 5 + inside)

    def tell(which, peer):
        pl.semaphore_signal(entered.at[which], inc=1, device_id=peer, device_id_type=MESH)

    @pl.when(inside == 1)
    def _():
        tell(0, at_plane(z1))
        tell(0, at_plane(outer))

    started = []

    def copy(src, dst, sems, recvs, peer):
        return pltpu.make_async_remote_copy(
            src_ref=src, dst_ref=dst, send_sem=sems, recv_sem=recvs,
            device_id=peer, device_id_type=MESH,
        )

    def send_between(src, dst, kind, there, here, peer):
        c = copy(src, dst, send_sem.at[kind, there], recv_sem.at[kind, here], peer)
        c.start()
        started.append(c)

    def send(block, kind, zz, peer):
        send_between(block, block, kind, zz, zz, peer)

    def arrived(dst, kind, zz):
        copy(dst, dst, send_sem.at[kind, zz], recv_sem.at[kind, zz], core_peer).wait_recv()

    low, high = pl.ds(0, half), pl.ds(half, half)

    def to_plane(zz):
        for part, kind in ((low, TO_PLANE), (high, TO_PLANE_2)):
            send_between(outgoing.at[zz, part], rows.at[q, x, z, part], kind, zz, z, at_plane(zz))

    def spread_low(zz):
        block = rows.at[q, x, zz]
        arrived(block.at[low], TO_PLANE, zz)
        send(block.at[low], ACROSS_X, zz, x_peer)
        send(block.at[low], ACROSS_Y2, zz, y_peer)

    def spread_high(zz):
        block = rows.at[q, x, zz]
        arrived(block.at[high], TO_PLANE_2, zz)
        send(block.at[high], ACROSS_Y, zz, y_peer)
        send(block.at[high], ACROSS_X2, zz, x_peer)
        send(block, CORE_OWN, zz, core_peer)

    def spread_own():
        block = rows.at[q, x, z]
        send(block.at[low], ACROSS_X, z, x_peer)
        send(block.at[high], ACROSS_Y, z, y_peer)
        send(block.at[high], ACROSS_X2, z, x_peer)
        send(block.at[low], ACROSS_Y2, z, y_peer)
        send(block, CORE_OWN, z, core_peer)

    def pass_on(zz):
        over_x, over_y = rows.at[q, ox, zz], rows.at[q_y, x, zz]
        arrived(over_x.at[low], ACROSS_X, zz)
        send(over_x.at[low], RELAY_Y, zz, y_peer)
        arrived(over_y.at[high], ACROSS_Y, zz)
        send(over_y.at[high], RELAY_X, zz, x_peer)
        arrived(over_x.at[high], ACROSS_X2, zz)
        send(over_x, CORE_X, zz, core_peer)
        arrived(over_y.at[low], ACROSS_Y2, zz)
        send(over_y, CORE_Y, zz, core_peer)

    def pass_relayed(zz):
        block = rows.at[q_y, ox, zz]
        arrived(block.at[low], RELAY_Y, zz)
        send(block.at[low], CORE_RY, zz, core_peer)
        arrived(block.at[high], RELAY_X, zz)
        send(block.at[high], CORE_RX, zz, core_peer)

    def sums_of(zz, quarter):
        part = jnp.concatenate([rows[quarter, x, zz], rows[quarter, ox, zz]], axis=0)
        w = w_in[pl.ds(pl.multiple_of(quarter * width, width), width), :]
        return jnp.dot(part, w, preferred_element_type=F32)

    def make_hidden(zz):
        total = sums_of(zz, q) + sums_of(zz, q_y)
        arrived(rows.at[q_core, x, zz], CORE_OWN, zz)
        arrived(rows.at[q_core, ox, zz], CORE_X, zz)
        total = total + sums_of(zz, q_core)
        arrived(rows.at[q_diag, x, zz], CORE_Y, zz)
        block = rows.at[q_diag, ox, zz]
        arrived(block.at[low], CORE_RY, zz)
        arrived(block.at[high], CORE_RX, zz)
        total = total + sums_of(zz, q_diag)
        gate, up = total[:, :inner], total[:, inner:]
        hidden[zz, q] = (gate / (1.0 + jnp.exp(-gate)) * up).astype(BF16)
        block = hidden.at[zz, q]
        for d, peer in ((2, y_peer), (3, diag_peer), (1, core_peer)):
            c = copy(block, block, hidden_send.at[d, zz], hidden_recv.at[d, zz], peer)
            c.start()
            started.append(c)

    lane = lax.broadcasted_iota(jnp.int32, (cap, 128), 1)
    place = lax.broadcasted_iota(jnp.int32, (cap, 128), 0) + z * cap
    here = lane == place
    none = jnp.zeros((cap, 128), F32)

    def column_of(row):
        return jnp.sum(jnp.where(here, jnp.broadcast_to(row, (cap, 128)), none), axis=1, keepdims=True)

    is_first = x == 0

    def project(zz):
        even_share, odd_share = column_of(share_in[zz, 0:1]), column_of(share_in[zz, 1:2])
        share_own = jnp.where(is_first, even_share, odd_share)
        share_far[zz] = jnp.broadcast_to(jnp.where(is_first, odd_share, even_share), (cap, 128))
        for d in range(1, n_tp):
            block = hidden.at[zz, flip(q, d)]
            copy(block, block, hidden_send.at[d, zz], hidden_recv.at[d, zz], core_peer).wait_recv()
        h = jnp.concatenate([hidden[zz, t] for t in range(n_tp)], axis=1)
        result = jnp.dot(h, w_out[...], preferred_element_type=F32).astype(BF16)
        result_out[zz] = result[cap:]
        for part, kind in ((low, RESULT), (high, RESULT_2)):
            send_between(result_out.at[zz, part], result_in.at[zz, part], kind, zz, zz, x_peer)
        own_part[zz] = result[:cap].astype(F32) * share_own

    def give_back(zz, own=False):
        for part, at, kind, home in ((low, 0, RESULT, BACK), (high, half, RESULT_2, BACK_2)):
            arrived(result_in.at[zz, part], kind, zz)
            scaled = result_in[zz, at:at + half].astype(F32) * share_far[zz, at:at + half][:, 0:1]
            routed = (own_part[zz, at:at + half] + scaled).astype(BF16)
            if own:
                back_in[z, at:at + half] = routed
            else:
                back_out[zz, at:at + half] = routed
                send_between(
                    back_out.at[zz, part], back_in.at[z, part], home, zz, z, at_plane(zz)
                )
        routed = back_in[z] if own else back_out[zz]
        mixed = residual_scale * rows[q, x, zz].astype(F32) + routed.astype(F32)
        total = jnp.sum(mixed, axis=1, keepdims=True)
        centered = mixed - total / width
        square = jnp.sum(centered * centered, axis=1, keepdims=True)
        for k, column in enumerate((total, square)):
            stats_out[zz, k:k + 1] = jnp.sum(
                jnp.where(here, jnp.broadcast_to(column, (cap, 128)), none), axis=0, keepdims=True
            )
        for d in (2, 3, 1, 0):
            if own and not d:
                stats_in[z, q] = stats_out[z]
                continue
            c = copy(
                stats_out.at[zz], stats_in.at[z, q], stats_send.at[d, zz], stats_recv.at[d, z],
                (zz * 2 + x, flip(q, d)),
            )
            c.start()
            started.append(c)

    to_plane(z1)
    spread_own()
    pl.semaphore_wait(entered.at[0], 1)

    @pl.when(inside == 1)
    def _():
        tell(1, at_plane(outer))

    to_plane(z2)

    @pl.when(inside == 0)
    def _():
        pl.semaphore_wait(entered.at[1], 1)

    to_plane(z3)
    for zz in (z1, z2, z3):
        send_between(share_out, share_in.at[z], SHARES, zz, z, at_plane(zz))

    spread_low(z1)
    pass_on(z)
    spread_high(z1)
    spread_low(z2)
    spread_high(z2)
    loads[0].wait()
    loads[1].wait()
    pass_relayed(z)
    pass_on(z1)
    make_hidden(z)
    pass_relayed(z1)
    pass_on(z2)
    spread_low(z3)
    spread_high(z3)
    make_hidden(z1)
    loads[2].wait()
    for zz in (z1, z2, z3):
        arrived(share_in.at[zz], SHARES, zz)
    pass_relayed(z2)
    project(z)
    pass_on(z3)
    make_hidden(z2)
    project(z1)
    pass_relayed(z3)
    give_back(z, own=True)
    make_hidden(z3)
    project(z2)
    give_back(z1)
    project(z3)
    give_back(z2)
    give_back(z3)

    for zz in (z1, z2, z3):
        arrived(back_in.at[zz, low], BACK, zz)
        arrived(back_in.at[zz, high], BACK_2, zz)
    routed = jnp.dot(
        jnp.where(to_token, one, zero).astype(BF16),
        back_in[...].reshape(tok, width),
        preferred_element_type=F32,
    )
    mixed = residual_scale * tokens_ref[...].astype(F32) + routed
    for d in range(n_tp):
        for zz in (z, z1, z2, z3) if d else (z1, z2, z3):
            block = stats_in.at[zz, flip(q, d)]
            copy(block, block, stats_send.at[d, zz], stats_recv.at[d, zz], core_peer).wait_recv()
    pieces = [sum(stats_in[zz, t] for zz in range(n_plane)) for t in range(n_tp)]
    full = width * n_tp
    center = sum(p[0:1] for p in pieces) / full
    spread = sum(p[1:2] + width * jnp.square(p[0:1] / width - center) for p in pieces) / full
    scale = lax.rsqrt(spread + norm_eps)
    center, scale = (
        jnp.sum(jnp.where(to_token, jnp.broadcast_to(row, (tok, tok)), zero), axis=1, keepdims=True)
        for row in (center, scale)
    )
    inputs[4].wait()
    inputs[5].wait()
    normed_out[...] = (
        (mixed - center) * scale * gain_ref[...] + bias_ref[...]
    ).astype(BF16)
    for c in started:
        c.wait_send()


def pair_groups(
    tokens, expert_ids, group_weight, expert_weight, w_gate, w_up, w_down, norm_gain, norm_bias
):
    tok, width = tokens.shape
    n_plane = lax.axis_size("ep") // TOP_K
    n_tp = lax.axis_size("tp")
    cap = tok // n_plane
    inner = w_gate.shape[2]
    vmem = pl.BlockSpec(memory_space=pltpu.VMEM)
    hbm = pl.BlockSpec(memory_space=pltpu.HBM)
    return pl.pallas_call(
        functools.partial(layer_kernel, n_plane, n_tp),
        out_shape=jax.ShapeDtypeStruct((tok, width), BF16),
        in_specs=[hbm] * 9,
        out_specs=vmem,
        scratch_shapes=[
            pltpu.VMEM((tok, width), BF16),
            pltpu.VMEM((TOP_K, tok), jnp.int32),
            pltpu.VMEM((1, tok), F32),
            pltpu.VMEM((TOP_K, tok), F32),
            pltpu.VMEM((1, width), F32),
            pltpu.VMEM((1, width), F32),
            pltpu.VMEM((w_gate.shape[1], 2 * inner), BF16),
            pltpu.VMEM(w_down.shape[1:], BF16),
            pltpu.VMEM((n_plane, cap, width), BF16),
            pltpu.VMEM((2, tok), F32),
            pltpu.VMEM((n_plane, 2, tok), F32),
            pltpu.VMEM((n_plane, cap, 128), F32),
            pltpu.VMEM((n_tp, 2, n_plane, cap, width), BF16),
            pltpu.VMEM((n_plane, n_tp, 2 * cap, inner), BF16),
            pltpu.VMEM((n_plane, cap, width), F32),
            pltpu.VMEM((n_plane, cap, width), BF16),
            pltpu.VMEM((n_plane, cap, width), BF16),
            pltpu.VMEM((n_plane, cap, width), BF16),
            pltpu.VMEM((n_plane, cap, width), BF16),
            pltpu.VMEM((n_plane, 2, tok), F32),
            pltpu.VMEM((n_plane, n_tp, 2, tok), F32),
            pltpu.SemaphoreType.DMA((KINDS, n_plane)),
            pltpu.SemaphoreType.DMA((KINDS, n_plane)),
            pltpu.SemaphoreType.DMA((n_tp, n_plane)),
            pltpu.SemaphoreType.DMA((n_tp, n_plane)),
            pltpu.SemaphoreType.DMA((n_tp, n_plane)),
            pltpu.SemaphoreType.DMA((n_tp, n_plane)),
            pltpu.SemaphoreType.DMA((9,)),
            pltpu.SemaphoreType.REGULAR((2,)),
        ],
        compiler_params=pltpu.CompilerParams(
            collective_id=0, has_side_effects=True, vmem_limit_bytes=53 * 2**20
        ),
        name="layer",
    )(
        *(
            pltpu.with_memory_space_constraint(a, pltpu.HBM)
            for a in (
                tokens, expert_ids.T, group_weight[None, :], expert_weight.T, w_gate, w_up, w_down,
                norm_gain[None, :], norm_bias[None, :],
            )
        )
    )


def solution(mesh):
    n_ep, n_tp = mesh.shape["ep"], mesh.shape["tp"]
    pairs = TOP_K == 2 and n_ep == GROUPS * TOP_K and n_tp == 4
    return jax.shard_map(
        pair_groups if pairs else on_device,
        mesh=mesh,
        in_specs=(
            P("ep", "tp"),
            P("ep", None),
            P("ep"),
            P("ep", None),
            P("ep", None, "tp"),
            P("ep", None, "tp"),
            P("ep", None, "tp"),
            P("tp"),
            P("tp"),
        ),
        out_specs=P("ep", "tp"),
        check_vma=False,
    )
```

```python
import functools

import jax
import jax.numpy as jnp
from jax import lax
from jax.experimental import pallas as pl
from jax.experimental.pallas import tpu as pltpu
from jax.sharding import PartitionSpec as P

D = 4096
GROUPS = 4
TOP_K = 2


residual_scale = 2.0**0.5
norm_eps = 1e-05


def on_device(
    tokens, expert_ids, group_weight, expert_weight, w_gate, w_up, w_down, norm_gain, norm_bias
):
    tok_count = tokens.shape[0]
    expert_count = lax.axis_size("ep")
    capacity = min(tok_count // GROUPS, 3 * TOP_K * tok_count // (2 * expert_count))
    pair_count = tok_count * TOP_K
    flat_ids = expert_ids.reshape(pair_count)
    one_hot = (flat_ids[:, None] == jnp.arange(expert_count, dtype=jnp.int32)[None, :]).astype(
        jnp.float32
    )
    earlier = (jnp.arange(pair_count)[:, None] > jnp.arange(pair_count)[None, :]).astype(
        jnp.float32
    )
    prior_counts = jnp.dot(
        earlier, one_hot, preferred_element_type=jnp.float32, precision=lax.Precision.HIGHEST
    )
    slot_index = jnp.sum(prior_counts * one_hot, axis=1).astype(jnp.int32)
    position = flat_ids * capacity + slot_index
    owner_token = jnp.arange(pair_count, dtype=jnp.int32) // TOP_K
    slot_table = (
        jnp.full((expert_count * capacity,), tok_count, jnp.int32).at[position].set(owner_token)
    )
    gate_local = w_gate[0]
    up_local = w_up[0]
    down_local = w_down[0]
    padded = jnp.concatenate([tokens, jnp.zeros((1, tokens.shape[1]), tokens.dtype)], axis=0)
    outgoing = padded[slot_table].reshape(expert_count, capacity, tokens.shape[1])
    arrived = lax.all_to_all(outgoing, "ep", split_axis=0, concat_axis=0, tiled=True)
    sources, slot_count, slice_width = arrived.shape
    row_block = arrived.reshape(sources * slot_count, slice_width)
    row_piece = lax.all_gather(row_block, "tp", axis=1, tiled=True)
    gate_sum = jnp.dot(row_piece, gate_local, preferred_element_type=jnp.float32)
    up_sum = jnp.dot(row_piece, up_local, preferred_element_type=jnp.float32)
    hidden = (jax.nn.silu(gate_sum) * up_sum).astype(jnp.bfloat16)
    result = jnp.dot(
        lax.all_gather(hidden, "tp", axis=1, tiled=True),
        down_local,
        preferred_element_type=jnp.float32,
    )
    result = result.astype(jnp.bfloat16).reshape(sources, slot_count, down_local.shape[1])
    returned = lax.all_to_all(result, "ep", split_axis=0, concat_axis=0, tiled=True)
    flat_rows = returned.reshape(expert_count * capacity, returned.shape[2])
    picked = flat_rows[position].reshape(tok_count, TOP_K, returned.shape[2]).astype(jnp.float32)
    share_weight = (
        group_weight[:, None] * expert_weight / jnp.sum(expert_weight, axis=1, keepdims=True)
    )
    routed = jnp.einsum("tk,tkd->td", share_weight, picked)
    mixed = residual_scale * tokens.astype(jnp.float32) + routed
    first_sum, second_sum = lax.psum((jnp.sum(mixed, axis=1), jnp.sum(mixed * mixed, axis=1)), "tp")
    center = first_sum / D
    spread = second_sum / D - center * center
    centered = mixed - center[:, None]
    normed = (
        centered * lax.rsqrt(spread + norm_eps)[:, None] * norm_gain[None, :] + norm_bias[None, :]
    )
    return normed.astype(jnp.bfloat16)


MESH = pl.DeviceIdType.MESH
F32 = jnp.float32
BF16 = jnp.bfloat16
(TO_PLANE, TO_PLANE_2, ACROSS_X, ACROSS_Y, ACROSS_X2, ACROSS_Y2, RELAY_X, RELAY_Y, CORE, HIDDEN,
 RESULT, RESULT_2) = range(12)
KINDS = 12
BACK, SHARES, STATS = range(3)
TO_CORE, IN_PLANE, OFF_PLANE, RESULTS, HIDDENS, SHARE, STAT = range(7)


def flip(value, bits):
    bit = 1
    while bit <= bits:
        if bits & bit:
            value = value + bit - 2 * bit * lax.rem(lax.div(value, bit), 2)
        bit *= 2
    return value


def layer_kernel(
    n_plane, n_tp,
    tokens_hbm, ids_hbm, group_hbm, expert_hbm, gate_hbm, up_hbm, down_hbm, gain_hbm, bias_hbm,
    normed_out,
    tokens_ref, ids_ref, group_ref, expert_ref, gain_ref, bias_ref,
    w_in, w_out, outgoing, share_out, share_in, share_far, rows, hidden, own_part, result_out,
    result_in, back_out, back_in, stats_out, stats_in,
    send_sem, recv_sem, once_sem, load_sem, entered,
):
    ep = lax.axis_index("ep")
    q = lax.axis_index("tp")
    z, x = lax.div(ep, 2), lax.rem(ep, 2)
    ox = 1 - x
    q_core, q_y, q_diag = flip(q, 1), flip(q, 2), flip(q, 3)
    core_peer, y_peer, diag_peer = (ep, q_core), (ep, q_y), (ep, q_diag)
    x_peer = (z * 2 + ox, q)

    def at_plane(zz):
        return (zz * 2 + x, q)

    last = n_plane - 1
    bottom = lax.div(last - z, last)
    t1 = bottom
    t2 = n_plane // 2 - lax.div(z, 2)
    t3 = last - lax.div(z, last)
    z1 = z - 1 + 2 * bottom
    z3 = last - last * lax.div(z, last)
    z2 = n_plane * last // 2 - z - z1 - z3

    tok, width = tokens_ref.shape
    cap = tok // n_plane
    half = cap // 2
    inner = gate_hbm.shape[2]

    inputs = [
        pltpu.make_async_copy(source, target, load_sem.at[3 + i])
        for i, (source, target) in enumerate((
            (ids_hbm, ids_ref), (tokens_hbm, tokens_ref), (group_hbm, group_ref),
            (expert_hbm, expert_ref), (gain_hbm, gain_ref), (bias_hbm, bias_ref),
        ))
    ]
    for load in inputs:
        load.start()

    barrier = pltpu.get_barrier_semaphore()
    for peer in (x_peer, core_peer, y_peer, diag_peer):
        pl.semaphore_signal(barrier, inc=1, device_id=peer, device_id_type=MESH)
    for zz in range(n_plane):

        @pl.when((zz > z) | (zz == z - 1))
        def _(zz=zz):
            pl.semaphore_signal(barrier, inc=1, device_id=at_plane(zz), device_id_type=MESH)

    def tell(which, peer):
        pl.semaphore_signal(entered.at[which], inc=1, device_id=peer, device_id_type=MESH)

    loads = [
        pltpu.make_async_copy(gate_hbm.at[0], w_in.at[:, pl.ds(0, inner)], load_sem.at[0]),
        pltpu.make_async_copy(up_hbm.at[0], w_in.at[:, pl.ds(inner, inner)], load_sem.at[1]),
        pltpu.make_async_copy(down_hbm.at[0], w_out, load_sem.at[2]),
    ]
    for load in loads:
        load.start()

    @pl.when(z == last)
    def _():
        pl.semaphore_wait(barrier, n_tp + last)
        tell(1, at_plane(0))
        tell(0, at_plane(1))

    inputs[0].wait()
    first = ids_ref[0:1, :]
    group_row = (first >> 1).astype(F32)
    on_lanes = jnp.broadcast_to(group_row, (tok, tok))
    on_rows = jnp.transpose(on_lanes)
    ii = lax.broadcasted_iota(jnp.int32, (tok, tok), 0)
    jj = lax.broadcasted_iota(jnp.int32, (tok, tok), 1)
    same = on_lanes == on_rows
    zero, one = jnp.zeros((tok, tok), F32), jnp.ones((tok, tok), F32)
    rank_row = jnp.sum(jnp.where(same & (ii < jj), one, zero), axis=0, keepdims=True)
    rank_col = jnp.sum(jnp.where(same & (jj < ii), one, zero), axis=1, keepdims=True)
    place_row = group_row * cap + rank_row
    place_col = on_rows[:, 0:1] * cap + rank_col
    to_slot = jnp.broadcast_to(place_row, (tok, tok)) == ii.astype(F32)
    to_token = jnp.broadcast_to(place_col, (tok, tok)) == jj.astype(F32)

    inputs[1].wait()
    sorted_rows = jnp.dot(
        jnp.where(to_slot, one, zero).astype(BF16), tokens_ref[...], preferred_element_type=F32
    ).astype(BF16)
    outgoing[...] = sorted_rows.reshape(n_plane, cap, width)
    rows[q, x, z] = outgoing[z]

    @pl.when(z < last)
    def _():
        pl.semaphore_wait(barrier, n_tp + 1 + z)

    @pl.when(z == 1)
    def _():
        tell(0, at_plane(0))

    def start(src, dst, group, arrival, peer):
        pltpu.make_async_remote_copy(
            src_ref=src, dst_ref=dst, send_sem=send_sem.at[group], recv_sem=arrival,
            device_id=peer, device_id_type=MESH,
        ).start()

    def send(block, kind, zz, peer, group=IN_PLANE):
        start(block, block, group, recv_sem.at[kind, zz], peer)

    def landed(ref, arrival):
        pltpu.make_async_copy(ref, ref, arrival).wait()

    def arrived(ref, kind, zz):
        landed(ref, recv_sem.at[kind, zz])

    low, high = pl.ds(0, half), pl.ds(half, half)

    def to_plane(zz):
        for part, kind in ((low, TO_PLANE), (high, TO_PLANE_2)):
            start(
                outgoing.at[zz, part], rows.at[q, x, z, part], OFF_PLANE, recv_sem.at[kind, z],
                at_plane(zz),
            )

    def spread_low(zz):
        block = rows.at[q, x, zz]
        arrived(block.at[low], TO_PLANE, zz)
        send(block.at[low], ACROSS_X, zz, x_peer)
        send(block.at[low], ACROSS_Y2, zz, y_peer)

    def spread_high(zz):
        block = rows.at[q, x, zz]
        arrived(block.at[high], TO_PLANE_2, zz)
        send(block.at[high], ACROSS_Y, zz, y_peer)
        send(block.at[high], ACROSS_X2, zz, x_peer)
        send(block, CORE, zz, core_peer, TO_CORE)

    def spread_own():
        block = rows.at[q, x, z]
        send(block.at[low], ACROSS_X, z, x_peer)
        send(block.at[high], ACROSS_Y, z, y_peer)
        send(block.at[high], ACROSS_X2, z, x_peer)
        send(block.at[low], ACROSS_Y2, z, y_peer)
        send(block, CORE, z, core_peer, TO_CORE)

    def pass_on(zz):
        over_x, over_y = rows.at[q, ox, zz], rows.at[q_y, x, zz]
        arrived(over_x.at[low], ACROSS_X, zz)
        send(over_x.at[low], RELAY_Y, zz, y_peer)
        arrived(over_y.at[high], ACROSS_Y, zz)
        send(over_y.at[high], RELAY_X, zz, x_peer)
        arrived(over_x.at[high], ACROSS_X2, zz)
        send(over_x, CORE, zz, core_peer, TO_CORE)
        arrived(over_y.at[low], ACROSS_Y2, zz)
        send(over_y, CORE, zz, core_peer, TO_CORE)

    def pass_relayed(zz):
        block = rows.at[q_y, ox, zz]
        arrived(block.at[low], RELAY_Y, zz)
        send(block.at[low], CORE, zz, core_peer, TO_CORE)
        arrived(block.at[high], RELAY_X, zz)
        send(block.at[high], CORE, zz, core_peer, TO_CORE)

    def sums_of(blocks, quarter):
        part = jnp.concatenate(
            [rows[quarter, column, zz] for zz in blocks for column in (x, ox)], axis=0
        )
        w = w_in[pl.ds(pl.multiple_of(quarter * width, width), width), :]
        return jnp.dot(part, w, preferred_element_type=F32)

    def make_hidden(*blocks):
        total = sums_of(blocks, q) + sums_of(blocks, q_y)
        for zz in blocks:
            arrived(rows.at[pl.ds(0, 2), :, zz], CORE, zz)
        total = total + sums_of(blocks, q_core) + sums_of(blocks, q_diag)
        gate, up = total[:, :inner], total[:, inner:]
        made = (gate / (1.0 + jnp.exp(-gate)) * up).astype(BF16)
        for i, zz in enumerate(blocks):
            hidden[zz, q] = made[2 * cap * i:2 * cap * (i + 1)]
            block = hidden.at[zz, q]
            for peer in (y_peer, diag_peer, core_peer):
                send(block, HIDDEN, zz, peer, HIDDENS)

    lane = lax.broadcasted_iota(jnp.int32, (cap, 128), 1)
    place = lax.broadcasted_iota(jnp.int32, (cap, 128), 0) + z * cap
    here = lane == place
    none = jnp.zeros((cap, 128), F32)

    def column_of(row):
        return jnp.sum(jnp.where(here, jnp.broadcast_to(row, (cap, 128)), none), axis=1, keepdims=True)

    is_first = x == 0

    def project(*blocks):
        for zz in blocks:
            arrived(hidden.at[zz, pl.ds(0, n_tp - 1)], HIDDEN, zz)
        h = jnp.concatenate(
            [
                jnp.concatenate([hidden[zz, t] for t in range(n_tp)], axis=1)
                for zz in blocks
            ],
            axis=0,
        )
        result = jnp.dot(h, w_out[...], preferred_element_type=F32).astype(BF16)
        for i, zz in enumerate(blocks):
            at = 2 * cap * i
            result_out[zz] = result[at + cap:at + 2 * cap]
            for part, kind in ((low, RESULT), (high, RESULT_2)):
                start(
                    result_out.at[zz, part], result_in.at[zz, part], RESULTS,
                    recv_sem.at[kind, zz], x_peer,
                )
        for i, zz in enumerate(blocks):
            at = 2 * cap * i
            even_share, odd_share = column_of(share_in[zz, 0:1]), column_of(share_in[zz, 1:2])
            share_own = jnp.where(is_first, even_share, odd_share)
            share_far[zz] = jnp.broadcast_to(jnp.where(is_first, odd_share, even_share), (cap, 128))
            own_part[zz] = result[at:at + cap].astype(F32) * share_own

    def give_back(zz, own=False):
        for part, at, kind in ((low, 0, RESULT), (high, half, RESULT_2)):
            arrived(result_in.at[zz, part], kind, zz)
            scaled = result_in[zz, at:at + half].astype(F32) * share_far[zz, at:at + half][:, 0:1]
            routed = (own_part[zz, at:at + half] + scaled).astype(BF16)
            if own:
                back_in[z, at:at + half] = routed
            else:
                back_out[zz, at:at + half] = routed
                start(
                    back_out.at[zz, part], back_in.at[z, part], OFF_PLANE, once_sem.at[BACK],
                    at_plane(zz),
                )
        routed = back_in[z] if own else back_out[zz]
        mixed = residual_scale * rows[q, x, zz].astype(F32) + routed.astype(F32)
        total = jnp.sum(mixed, axis=1, keepdims=True)
        centered = mixed - total / width
        square = jnp.sum(centered * centered, axis=1, keepdims=True)
        for k, column in enumerate((total, square)):
            stats_out[zz, k:k + 1] = jnp.sum(
                jnp.where(here, jnp.broadcast_to(column, (cap, 128)), none), axis=0, keepdims=True
            )
        for d in (2, 3, 1, 0):
            if own and not d:
                stats_in[z * n_tp + q] = stats_out[z]
                continue
            start(
                stats_out.at[zz], stats_in.at[z * n_tp + q], STAT, once_sem.at[STATS],
                (zz * 2 + x, flip(q, d)),
            )

    def make_shares():
        inputs[2].wait()
        inputs[3].wait()
        weights = expert_ref[...]
        share = group_ref[...] * weights / jnp.sum(weights, axis=0, keepdims=True)
        even = (first & 1) == 0
        for k in range(2):
            chosen = jnp.where(even, share[k:k + 1, :], share[1 - k:2 - k, :])
            by_token = jnp.transpose(jnp.broadcast_to(chosen, (tok, tok)))
            share_out[k:k + 1, :] = jnp.sum(jnp.where(to_token, by_token, zero), axis=0, keepdims=True)
        share_in[z] = share_out[...]
        for zz in (z1, z2, z3):
            start(share_out, share_in.at[z], SHARE, once_sem.at[SHARES], at_plane(zz))

    to_plane(t1)
    spread_own()

    @pl.when(z == 0)
    def _():
        pl.semaphore_wait(entered.at[0], 1)

    to_plane(t2)

    @pl.when(z == 0)
    def _():
        pl.semaphore_wait(entered.at[1], 1)

    @pl.when(z == 1)
    def _():
        pl.semaphore_wait(entered.at[0], 1)

    to_plane(t3)
    spread_low(z1)
    pass_on(z)
    spread_high(z1)
    make_shares()
    spread_low(z2)
    spread_high(z2)
    pass_relayed(z)
    pass_on(z1)
    spread_low(z3)
    spread_high(z3)
    loads[0].wait()
    loads[1].wait()
    make_hidden(z)
    pass_relayed(z1)
    pass_on(z2)
    make_hidden(z1)
    pass_on(z3)
    loads[2].wait()
    landed(share_in.at[pl.ds(0, n_plane - 1)], once_sem.at[SHARES])
    project(z)
    pass_relayed(z2)
    make_hidden(z2)
    project(z1)
    pass_relayed(z3)
    make_hidden(z3)
    project(z2)
    give_back(z, own=True)
    give_back(z1)
    project(z3)
    give_back(z2)
    give_back(z3)

    landed(back_in.at[pl.ds(0, n_plane - 1)], once_sem.at[BACK])
    routed = jnp.dot(
        jnp.where(to_token, one, zero).astype(BF16),
        back_in[...].reshape(tok, width),
        preferred_element_type=F32,
    )
    mixed = residual_scale * tokens_ref[...].astype(F32) + routed
    landed(stats_in.at[pl.ds(0, n_plane * n_tp - 1)], once_sem.at[STATS])
    pieces = [sum(stats_in[zz * n_tp + t] for zz in range(n_plane)) for t in range(n_tp)]
    full = width * n_tp
    center = sum(p[0:1] for p in pieces) / full
    spread = sum(p[1:2] + width * jnp.square(p[0:1] / width - center) for p in pieces) / full
    scale = lax.rsqrt(spread + norm_eps)
    center, scale = (
        jnp.sum(jnp.where(to_token, jnp.broadcast_to(row, (tok, tok)), zero), axis=1, keepdims=True)
        for row in (center, scale)
    )
    inputs[4].wait()
    inputs[5].wait()
    normed_out[...] = (
        (mixed - center) * scale * gain_ref[...] + bias_ref[...]
    ).astype(BF16)
    for group, ref in (
        (TO_CORE, rows.at[pl.ds(0, 2)]),
        (IN_PLANE, rows.at[pl.ds(0, 3), 0]),
        (OFF_PLANE, rows.at[pl.ds(0, 2), 0, pl.ds(0, n_plane - 1)]),
        (RESULTS, result_out),
        (HIDDENS, hidden.at[:, pl.ds(0, n_tp - 1)]),
        (SHARE, share_in.at[pl.ds(0, n_plane - 1)]),
        (STAT, stats_in.at[pl.ds(0, n_plane * n_tp - 1)]),
    ):
        landed(ref, send_sem.at[group])


def pair_groups(
    tokens, expert_ids, group_weight, expert_weight, w_gate, w_up, w_down, norm_gain, norm_bias
):
    tok, width = tokens.shape
    n_plane = lax.axis_size("ep") // TOP_K
    n_tp = lax.axis_size("tp")
    cap = tok // n_plane
    inner = w_gate.shape[2]
    vmem = pl.BlockSpec(memory_space=pltpu.VMEM)
    hbm = pl.BlockSpec(memory_space=pltpu.HBM)
    return pl.pallas_call(
        functools.partial(layer_kernel, n_plane, n_tp),
        out_shape=jax.ShapeDtypeStruct((tok, width), BF16),
        in_specs=[hbm] * 9,
        out_specs=vmem,
        scratch_shapes=[
            pltpu.VMEM((tok, width), BF16),
            pltpu.VMEM((TOP_K, tok), jnp.int32),
            pltpu.VMEM((1, tok), F32),
            pltpu.VMEM((TOP_K, tok), F32),
            pltpu.VMEM((1, width), F32),
            pltpu.VMEM((1, width), F32),
            pltpu.VMEM((w_gate.shape[1], 2 * inner), BF16),
            pltpu.VMEM(w_down.shape[1:], BF16),
            pltpu.VMEM((n_plane, cap, width), BF16),
            pltpu.VMEM((2, tok), F32),
            pltpu.VMEM((n_plane, 2, tok), F32),
            pltpu.VMEM((n_plane, cap, 128), F32),
            pltpu.VMEM((n_tp, 2, n_plane, cap, width), BF16),
            pltpu.VMEM((n_plane, n_tp, 2 * cap, inner), BF16),
            pltpu.VMEM((n_plane, cap, width), F32),
            pltpu.VMEM((n_plane, cap, width), BF16),
            pltpu.VMEM((n_plane, cap, width), BF16),
            pltpu.VMEM((n_plane, cap, width), BF16),
            pltpu.VMEM((n_plane, cap, width), BF16),
            pltpu.VMEM((n_plane, 2, tok), F32),
            pltpu.VMEM((n_plane * n_tp, 2, tok), F32),
            pltpu.SemaphoreType.DMA((7,)),
            pltpu.SemaphoreType.DMA((KINDS, n_plane)),
            pltpu.SemaphoreType.DMA((3,)),
            pltpu.SemaphoreType.DMA((9,)),
            pltpu.SemaphoreType.REGULAR((2,)),
        ],
        compiler_params=pltpu.CompilerParams(
            collective_id=0, has_side_effects=True, vmem_limit_bytes=53 * 2**20
        ),
        name="layer",
    )(
        *(
            pltpu.with_memory_space_constraint(a, pltpu.HBM)
            for a in (
                tokens, expert_ids.T, group_weight[None, :], expert_weight.T, w_gate, w_up, w_down,
                norm_gain[None, :], norm_bias[None, :],
            )
        )
    )


def solution(mesh):
    n_ep, n_tp = mesh.shape["ep"], mesh.shape["tp"]
    pairs = TOP_K == 2 and n_ep == GROUPS * TOP_K and n_tp == 4
    return jax.shard_map(
        pair_groups if pairs else on_device,
        mesh=mesh,
        in_specs=(
            P("ep", "tp"),
            P("ep", None),
            P("ep"),
            P("ep", None),
            P("ep", None, "tp"),
            P("ep", None, "tp"),
            P("ep", None, "tp"),
            P("tp"),
            P("tp"),
        ),
        out_specs=P("ep", "tp"),
        check_vma=False,
    )
```

```python
import functools

import jax
import jax.numpy as jnp
from jax import lax
from jax.experimental import pallas as pl
from jax.experimental.pallas import tpu as pltpu
from jax.sharding import PartitionSpec as P

D = 4096
GROUPS = 4
TOP_K = 2


residual_scale = 2.0**0.5
norm_eps = 1e-05


def on_device(
    tokens, expert_ids, group_weight, expert_weight, w_gate, w_up, w_down, norm_gain, norm_bias
):
    tok_count = tokens.shape[0]
    expert_count = lax.axis_size("ep")
    capacity = min(tok_count // GROUPS, 3 * TOP_K * tok_count // (2 * expert_count))
    pair_count = tok_count * TOP_K
    flat_ids = expert_ids.reshape(pair_count)
    one_hot = (flat_ids[:, None] == jnp.arange(expert_count, dtype=jnp.int32)[None, :]).astype(
        jnp.float32
    )
    earlier = (jnp.arange(pair_count)[:, None] > jnp.arange(pair_count)[None, :]).astype(
        jnp.float32
    )
    prior_counts = jnp.dot(
        earlier, one_hot, preferred_element_type=jnp.float32, precision=lax.Precision.HIGHEST
    )
    slot_index = jnp.sum(prior_counts * one_hot, axis=1).astype(jnp.int32)
    position = flat_ids * capacity + slot_index
    owner_token = jnp.arange(pair_count, dtype=jnp.int32) // TOP_K
    slot_table = (
        jnp.full((expert_count * capacity,), tok_count, jnp.int32).at[position].set(owner_token)
    )
    gate_local = w_gate[0]
    up_local = w_up[0]
    down_local = w_down[0]
    padded = jnp.concatenate([tokens, jnp.zeros((1, tokens.shape[1]), tokens.dtype)], axis=0)
    outgoing = padded[slot_table].reshape(expert_count, capacity, tokens.shape[1])
    arrived = lax.all_to_all(outgoing, "ep", split_axis=0, concat_axis=0, tiled=True)
    sources, slot_count, slice_width = arrived.shape
    row_block = arrived.reshape(sources * slot_count, slice_width)
    row_piece = lax.all_gather(row_block, "tp", axis=1, tiled=True)
    gate_sum = jnp.dot(row_piece, gate_local, preferred_element_type=jnp.float32)
    up_sum = jnp.dot(row_piece, up_local, preferred_element_type=jnp.float32)
    hidden = (jax.nn.silu(gate_sum) * up_sum).astype(jnp.bfloat16)
    result = jnp.dot(
        lax.all_gather(hidden, "tp", axis=1, tiled=True),
        down_local,
        preferred_element_type=jnp.float32,
    )
    result = result.astype(jnp.bfloat16).reshape(sources, slot_count, down_local.shape[1])
    returned = lax.all_to_all(result, "ep", split_axis=0, concat_axis=0, tiled=True)
    flat_rows = returned.reshape(expert_count * capacity, returned.shape[2])
    picked = flat_rows[position].reshape(tok_count, TOP_K, returned.shape[2]).astype(jnp.float32)
    share_weight = (
        group_weight[:, None] * expert_weight / jnp.sum(expert_weight, axis=1, keepdims=True)
    )
    routed = jnp.einsum("tk,tkd->td", share_weight, picked)
    mixed = residual_scale * tokens.astype(jnp.float32) + routed
    first_sum, second_sum = lax.psum((jnp.sum(mixed, axis=1), jnp.sum(mixed * mixed, axis=1)), "tp")
    center = first_sum / D
    spread = second_sum / D - center * center
    centered = mixed - center[:, None]
    normed = (
        centered * lax.rsqrt(spread + norm_eps)[:, None] * norm_gain[None, :] + norm_bias[None, :]
    )
    return normed.astype(jnp.bfloat16)


MESH = pl.DeviceIdType.MESH
F32 = jnp.float32
BF16 = jnp.bfloat16
(FROM_LOWER, FROM_UPPER, ACROSS_X, ACROSS_Y, ACROSS_X2, ACROSS_Y2, RELAY_X, RELAY_Y, CORE, HIDDEN,
 RESULT, RESULT_2) = range(12)
KINDS = 12
BACK, SHARES, STATS = range(3)
TO_CORE, IN_PLANE, OFF_PLANE, RESULTS, HIDDENS, SHARE, STAT = range(7)


def flip(value, bits):
    bit = 1
    while bit <= bits:
        if bits & bit:
            value = value + bit - 2 * bit * lax.rem(lax.div(value, bit), 2)
        bit *= 2
    return value


def layer_kernel(
    n_plane, n_tp,
    tokens_hbm, ids_hbm, group_hbm, expert_hbm, gate_hbm, up_hbm, down_hbm, gain_hbm, bias_hbm,
    normed_out,
    tokens_ref, ids_ref, group_ref, expert_ref, gain_ref, bias_ref,
    w_in, w_out, outgoing, share_out, share_in, share_far, rows, hidden, own_part, result_out,
    result_in, back_out, back_in, stats_out, stats_in,
    send_sem, recv_sem, once_sem, load_sem, entered,
):
    ep = lax.axis_index("ep")
    q = lax.axis_index("tp")
    z, x = lax.div(ep, 2), lax.rem(ep, 2)
    ox = 1 - x
    q_core, q_y, q_diag = flip(q, 1), flip(q, 2), flip(q, 3)
    core_peer, y_peer, diag_peer = (ep, q_core), (ep, q_y), (ep, q_diag)
    x_peer = (z * 2 + ox, q)

    upper = lax.rem(q, 2)
    q_up = q - upper + 1
    q_low = q_up - 1
    q_up_y = flip(q_up, 2)
    q_low_y = q_up_y - 1

    def at_plane(zz):
        return (zz * 2 + x, q)

    last = n_plane - 1
    bottom = lax.div(last - z, last)
    t1 = bottom
    t2 = n_plane // 2 - lax.div(z, 2)
    t3 = last - lax.div(z, last)
    z1 = z - 1 + 2 * bottom
    z3 = last - 2 * lax.div(z, last)
    z2 = n_plane * last // 2 - z - z1 - z3

    w1 = z1 * (1 - lax.div(z, 2))
    w3 = z3
    w2 = n_plane * last // 2 - z - w1 - w3

    tok, width = tokens_ref.shape
    cap = tok // n_plane
    half = cap // 2
    inner = gate_hbm.shape[2]

    inputs = [
        pltpu.make_async_copy(source, target, load_sem.at[3 + i])
        for i, (source, target) in enumerate((
            (ids_hbm, ids_ref), (tokens_hbm, tokens_ref), (group_hbm, group_ref),
            (expert_hbm, expert_ref), (gain_hbm, gain_ref), (bias_hbm, bias_ref),
        ))
    ]
    for load in inputs:
        load.start()

    barrier = pltpu.get_barrier_semaphore()
    for peer in (x_peer, core_peer, y_peer, diag_peer):
        pl.semaphore_signal(barrier, inc=1, device_id=peer, device_id_type=MESH)
    for zz in range(n_plane):

        @pl.when((zz > z) | (zz == z - 1))
        def _(zz=zz):
            for peer in (at_plane(zz), (zz * 2 + x, q_core)):
                pl.semaphore_signal(barrier, inc=1, device_id=peer, device_id_type=MESH)

    def tell(which, peer):
        pl.semaphore_signal(entered.at[which], inc=1, device_id=peer, device_id_type=MESH)

    loads = [
        pltpu.make_async_copy(gate_hbm.at[0], w_in.at[:, pl.ds(0, inner)], load_sem.at[0]),
        pltpu.make_async_copy(up_hbm.at[0], w_in.at[:, pl.ds(inner, inner)], load_sem.at[1]),
        pltpu.make_async_copy(down_hbm.at[0], w_out, load_sem.at[2]),
    ]
    for load in loads:
        load.start()

    @pl.when(z == last)
    def _():
        pl.semaphore_wait(barrier, n_tp + 2 * last)
        tell(1, at_plane(0))
        tell(0, at_plane(1))

    inputs[0].wait()
    first = ids_ref[0:1, :]
    group_row = (first >> 1).astype(F32)
    on_lanes = jnp.broadcast_to(group_row, (tok, tok))
    on_rows = jnp.transpose(on_lanes)
    ii = lax.broadcasted_iota(jnp.int32, (tok, tok), 0)
    jj = lax.broadcasted_iota(jnp.int32, (tok, tok), 1)
    same = on_lanes == on_rows
    zero, one = jnp.zeros((tok, tok), F32), jnp.ones((tok, tok), F32)
    rank_row = jnp.sum(jnp.where(same & (ii < jj), one, zero), axis=0, keepdims=True)
    rank_col = jnp.sum(jnp.where(same & (jj < ii), one, zero), axis=1, keepdims=True)
    place_row = group_row * cap + rank_row
    place_col = on_rows[:, 0:1] * cap + rank_col
    to_slot = jnp.broadcast_to(place_row, (tok, tok)) == ii.astype(F32)
    to_token = jnp.broadcast_to(place_col, (tok, tok)) == jj.astype(F32)

    inputs[1].wait()
    sorted_rows = jnp.dot(
        jnp.where(to_slot, one, zero).astype(BF16), tokens_ref[...], preferred_element_type=F32
    ).astype(BF16)
    outgoing[...] = sorted_rows.reshape(n_plane, cap, width)

    @pl.when(upper == 1)
    def _():
        rows[q, x, z] = outgoing[z]


    @pl.when(z < last)
    def _():
        pl.semaphore_wait(barrier, n_tp + 2 + 2 * z)

    @pl.when(z == 1)
    def _():
        tell(0, at_plane(0))

    def start(src, dst, group, arrival, peer):
        pltpu.make_async_remote_copy(
            src_ref=src, dst_ref=dst, send_sem=send_sem.at[group], recv_sem=arrival,
            device_id=peer, device_id_type=MESH,
        ).start()

    def send(block, kind, zz, peer, group=IN_PLANE):
        start(block, block, group, recv_sem.at[kind, zz], peer)

    def landed(ref, arrival):
        pltpu.make_async_copy(ref, ref, arrival).wait()

    def arrived(ref, kind, zz):
        landed(ref, recv_sem.at[kind, zz])

    low, high = pl.ds(0, half), pl.ds(half, half)

    def to_plane(zz):
        start(
            outgoing.at[zz], rows.at[q, x, z], OFF_PLANE, recv_sem.at[FROM_LOWER + upper, z],
            (zz * 2 + x, q_up),
        )

    def hand_over():
        start(outgoing.at[z], rows.at[q, x, z], TO_CORE, recv_sem.at[FROM_LOWER, z], core_peer)

    def to_core(block, zz):
        send(block, CORE, zz, core_peer, TO_CORE)

    def spread_up(zz):
        block = rows.at[q_up, x, zz]
        if zz is not z:
            arrived(block, FROM_UPPER, zz)
        send(block, ACROSS_X, zz, x_peer)
        send(block, ACROSS_Y2, zz, y_peer)
        to_core(block, zz)

    def spread_low(zz):
        block = rows.at[q_low, x, zz]
        arrived(block, FROM_LOWER, zz)
        send(block, ACROSS_Y, zz, y_peer)
        send(block, ACROSS_X2, zz, x_peer)
        to_core(block, zz)

    def pass_on(zz):
        block = rows.at[q_up, ox, zz]
        arrived(block, ACROSS_X, zz)
        send(block, RELAY_Y, zz, y_peer)
        to_core(block, zz)
        block = rows.at[q_low_y, x, zz]
        arrived(block, ACROSS_Y, zz)
        send(block, RELAY_X, zz, x_peer)
        to_core(block, zz)
        block = rows.at[q_low, ox, zz]
        arrived(block, ACROSS_X2, zz)
        to_core(block, zz)
        block = rows.at[q_up_y, x, zz]
        arrived(block, ACROSS_Y2, zz)
        to_core(block, zz)

    def pass_relayed(zz):
        for block, kind in (
            (rows.at[q_up_y, ox, zz], RELAY_Y), (rows.at[q_low_y, ox, zz], RELAY_X),
        ):
            arrived(block, kind, zz)
            to_core(block, zz)

    def sums_of(blocks, quarter):
        part = jnp.concatenate(
            [rows[quarter, column, zz] for zz in blocks for column in (x, ox)], axis=0
        )
        w = w_in[quarter * width:(quarter + 1) * width, :]
        return jnp.dot(part, w, preferred_element_type=F32)

    def make_hidden(*blocks, lower=False):
        if lower:
            for zz in blocks:
                arrived(rows.at[:, :, zz], CORE, zz)
        total = sum(sums_of(blocks, t) for t in range(n_tp))
        gate, up = total[:, :inner], total[:, inner:]
        made = (gate / (1.0 + jnp.exp(-gate)) * up).astype(BF16)
        for i, zz in enumerate(blocks):
            hidden[zz, q] = made[2 * cap * i:2 * cap * (i + 1)]
            block = hidden.at[zz, q]
            for peer in (y_peer, diag_peer, core_peer):
                send(block, HIDDEN, zz, peer, HIDDENS)

    lane = lax.broadcasted_iota(jnp.int32, (cap, 128), 1)
    place = lax.broadcasted_iota(jnp.int32, (cap, 128), 0) + z * cap
    here = lane == place
    none = jnp.zeros((cap, 128), F32)

    def column_of(row):
        return jnp.sum(jnp.where(here, jnp.broadcast_to(row, (cap, 128)), none), axis=1, keepdims=True)

    is_first = x == 0

    def project(*blocks):
        for zz in blocks:
            arrived(hidden.at[zz, pl.ds(0, n_tp - 1)], HIDDEN, zz)
        h = jnp.concatenate(
            [
                jnp.concatenate([hidden[zz, t] for t in range(n_tp)], axis=1)
                for zz in blocks
            ],
            axis=0,
        )
        result = jnp.dot(h, w_out[...], preferred_element_type=F32).astype(BF16)
        for i, zz in enumerate(blocks):
            at = 2 * cap * i
            result_out[zz] = result[at + cap:at + 2 * cap]
            for part, kind in ((low, RESULT), (high, RESULT_2)):
                start(
                    result_out.at[zz, part], result_in.at[zz, part], RESULTS,
                    recv_sem.at[kind, zz], x_peer,
                )
        for i, zz in enumerate(blocks):
            at = 2 * cap * i
            even_share, odd_share = column_of(share_in[zz, 0:1]), column_of(share_in[zz, 1:2])
            share_own = jnp.where(is_first, even_share, odd_share)
            share_far[zz] = jnp.broadcast_to(jnp.where(is_first, odd_share, even_share), (cap, 128))
            own_part[zz] = result[at:at + cap].astype(F32) * share_own

    def give_back(zz, own=False):
        for part, at, kind in ((low, 0, RESULT), (high, half, RESULT_2)):
            arrived(result_in.at[zz, part], kind, zz)
            scaled = result_in[zz, at:at + half].astype(F32) * share_far[zz, at:at + half][:, 0:1]
            routed = (own_part[zz, at:at + half] + scaled).astype(BF16)
            if own:
                back_in[z, at:at + half] = routed
            else:
                back_out[zz, at:at + half] = routed
                start(
                    back_out.at[zz, part], back_in.at[z, part], OFF_PLANE, once_sem.at[BACK],
                    at_plane(zz),
                )
        routed = back_in[z] if own else back_out[zz]
        mixed = residual_scale * rows[q, x, zz].astype(F32) + routed.astype(F32)
        total = jnp.sum(mixed, axis=1, keepdims=True)
        centered = mixed - total / width
        square = jnp.sum(centered * centered, axis=1, keepdims=True)
        for k, column in enumerate((total, square)):
            stats_out[zz, k:k + 1] = jnp.sum(
                jnp.where(here, jnp.broadcast_to(column, (cap, 128)), none), axis=0, keepdims=True
            )
        for d in (2, 3, 1, 0):
            if own and not d:
                stats_in[z * n_tp + q] = stats_out[z]
                continue
            start(
                stats_out.at[zz], stats_in.at[z * n_tp + q], STAT, once_sem.at[STATS],
                (zz * 2 + x, flip(q, d)),
            )

    def make_shares():
        inputs[2].wait()
        inputs[3].wait()
        weights = expert_ref[...]
        share = group_ref[...] * weights / jnp.sum(weights, axis=0, keepdims=True)
        even = (first & 1) == 0
        for k in range(2):
            chosen = jnp.where(even, share[k:k + 1, :], share[1 - k:2 - k, :])
            by_token = jnp.transpose(jnp.broadcast_to(chosen, (tok, tok)))
            share_out[k:k + 1, :] = jnp.sum(jnp.where(to_token, by_token, zero), axis=0, keepdims=True)
        share_in[z] = share_out[...]
        for zz in (z1, z2, z3):
            start(share_out, share_in.at[z], SHARE, once_sem.at[SHARES], at_plane(zz))

    to_plane(t1)

    @pl.when(upper == 1)
    def _():
        spread_up(z)

    @pl.when(upper == 0)
    def _():
        hand_over()

    @pl.when(z == 0)
    def _():
        pl.semaphore_wait(entered.at[0], 1)

    to_plane(t2)

    @pl.when(z >= 2)
    def _():
        to_plane(t3)

    @pl.when(upper == 1)
    def _():
        spread_low(z)

    @pl.when(z == 0)
    def _():
        pl.semaphore_wait(entered.at[1], 1)
        to_plane(t3)


    @pl.when(upper == 1)
    def _():
        spread_up(z1)
        pass_on(z)
        spread_low(z1)
        @pl.when(z == 1)
        def _():
            pl.semaphore_wait(entered.at[0], 1)
            to_plane(t3)

        make_shares()
        spread_up(z2)
        spread_low(z2)
        pass_relayed(z)
        pass_on(z1)
        spread_up(z3)
        spread_low(z3)
        loads[0].wait()
        loads[1].wait()
        make_hidden(z)
        pass_relayed(z1)
        pass_on(z2)
        make_hidden(z1)
        pass_on(z3)
        loads[2].wait()
        landed(share_in.at[pl.ds(0, n_plane - 1)], once_sem.at[SHARES])
        project(z)
        pass_relayed(z2)
        make_hidden(z2)
        pass_relayed(z3)
        make_hidden(z3)
        project(w1)
        project(w2)
        give_back(z, own=True)
        give_back(w1)
        project(w3)
        give_back(w2)
        give_back(w3)

    @pl.when(upper == 0)
    def _():
        @pl.when(z == 1)
        def _():
            pl.semaphore_wait(entered.at[0], 1)
            to_plane(t3)

        make_shares()
        loads[0].wait()
        loads[1].wait()
        make_hidden(z, lower=True)
        make_hidden(z1, lower=True)
        loads[2].wait()
        landed(share_in.at[pl.ds(0, n_plane - 1)], once_sem.at[SHARES])
        project(z)
        make_hidden(z2, lower=True)
        make_hidden(z3, lower=True)
        project(w1)
        project(w2)
        give_back(z, own=True)
        give_back(w1)
        project(w3)
        give_back(w2)
        give_back(w3)

    landed(back_in.at[pl.ds(0, n_plane - 1)], once_sem.at[BACK])
    routed = jnp.dot(
        jnp.where(to_token, one, zero).astype(BF16),
        back_in[...].reshape(tok, width),
        preferred_element_type=F32,
    )
    mixed = residual_scale * tokens_ref[...].astype(F32) + routed
    landed(stats_in.at[pl.ds(0, n_plane * n_tp - 1)], once_sem.at[STATS])
    pieces = [sum(stats_in[zz * n_tp + t] for zz in range(n_plane)) for t in range(n_tp)]
    full = width * n_tp
    center = sum(p[0:1] for p in pieces) / full
    spread = sum(p[1:2] + width * jnp.square(p[0:1] / width - center) for p in pieces) / full
    scale = lax.rsqrt(spread + norm_eps)
    center, scale = (
        jnp.sum(jnp.where(to_token, jnp.broadcast_to(row, (tok, tok)), zero), axis=1, keepdims=True)
        for row in (center, scale)
    )
    inputs[4].wait()
    inputs[5].wait()
    normed_out[...] = (
        (mixed - center) * scale * gain_ref[...] + bias_ref[...]
    ).astype(BF16)
    @pl.when(upper == 1)
    def _():
        landed(rows, send_sem.at[TO_CORE])
        landed(rows.at[pl.ds(0, n_tp - 1)], send_sem.at[IN_PLANE])

    @pl.when(upper == 0)
    def _():
        landed(outgoing.at[0], send_sem.at[TO_CORE])

    for group, ref in (
        (OFF_PLANE, rows.at[pl.ds(0, 2), 0, pl.ds(0, n_plane - 1)]),
        (RESULTS, result_out),
        (HIDDENS, hidden.at[:, pl.ds(0, n_tp - 1)]),
        (SHARE, share_in.at[pl.ds(0, n_plane - 1)]),
        (STAT, stats_in.at[pl.ds(0, n_plane * n_tp - 1)]),
    ):
        landed(ref, send_sem.at[group])


def pair_groups(
    tokens, expert_ids, group_weight, expert_weight, w_gate, w_up, w_down, norm_gain, norm_bias
):
    tok, width = tokens.shape
    n_plane = lax.axis_size("ep") // TOP_K
    n_tp = lax.axis_size("tp")
    cap = tok // n_plane
    inner = w_gate.shape[2]
    vmem = pl.BlockSpec(memory_space=pltpu.VMEM)
    hbm = pl.BlockSpec(memory_space=pltpu.HBM)
    return pl.pallas_call(
        functools.partial(layer_kernel, n_plane, n_tp),
        out_shape=jax.ShapeDtypeStruct((tok, width), BF16),
        in_specs=[hbm] * 9,
        out_specs=vmem,
        scratch_shapes=[
            pltpu.VMEM((tok, width), BF16),
            pltpu.VMEM((TOP_K, tok), jnp.int32),
            pltpu.VMEM((1, tok), F32),
            pltpu.VMEM((TOP_K, tok), F32),
            pltpu.VMEM((1, width), F32),
            pltpu.VMEM((1, width), F32),
            pltpu.VMEM((w_gate.shape[1], 2 * inner), BF16),
            pltpu.VMEM(w_down.shape[1:], BF16),
            pltpu.VMEM((n_plane, cap, width), BF16),
            pltpu.VMEM((2, tok), F32),
            pltpu.VMEM((n_plane, 2, tok), F32),
            pltpu.VMEM((n_plane, cap, 128), F32),
            pltpu.VMEM((n_tp, 2, n_plane, cap, width), BF16),
            pltpu.VMEM((n_plane, n_tp, 2 * cap, inner), BF16),
            pltpu.VMEM((n_plane, cap, width), F32),
            pltpu.VMEM((n_plane, cap, width), BF16),
            pltpu.VMEM((n_plane, cap, width), BF16),
            pltpu.VMEM((n_plane, cap, width), BF16),
            pltpu.VMEM((n_plane, cap, width), BF16),
            pltpu.VMEM((n_plane, 2, tok), F32),
            pltpu.VMEM((n_plane * n_tp, 2, tok), F32),
            pltpu.SemaphoreType.DMA((7,)),
            pltpu.SemaphoreType.DMA((KINDS, n_plane)),
            pltpu.SemaphoreType.DMA((3,)),
            pltpu.SemaphoreType.DMA((9,)),
            pltpu.SemaphoreType.REGULAR((2,)),
        ],
        compiler_params=pltpu.CompilerParams(
            collective_id=0, has_side_effects=True, vmem_limit_bytes=53 * 2**20
        ),
        name="layer",
    )(
        *(
            pltpu.with_memory_space_constraint(a, pltpu.HBM)
            for a in (
                tokens, expert_ids.T, group_weight[None, :], expert_weight.T, w_gate, w_up, w_down,
                norm_gain[None, :], norm_bias[None, :],
            )
        )
    )


def solution(mesh):
    n_ep, n_tp = mesh.shape["ep"], mesh.shape["tp"]
    pairs = TOP_K == 2 and n_ep == GROUPS * TOP_K and n_tp == 4
    return jax.shard_map(
        pair_groups if pairs else on_device,
        mesh=mesh,
        in_specs=(
            P("ep", "tp"),
            P("ep", None),
            P("ep"),
            P("ep", None),
            P("ep", None, "tp"),
            P("ep", None, "tp"),
            P("ep", None, "tp"),
            P("tp"),
            P("tp"),
        ),
        out_specs=P("ep", "tp"),
        check_vma=False,
    )
```

```python
import functools

import jax
import jax.numpy as jnp
from jax import lax
from jax.experimental import pallas as pl
from jax.experimental.pallas import tpu as pltpu
from jax.sharding import PartitionSpec as P

D = 4096
GROUPS = 4
TOP_K = 2


residual_scale = 2.0**0.5
norm_eps = 1e-05


def on_device(
    tokens, expert_ids, group_weight, expert_weight, w_gate, w_up, w_down, norm_gain, norm_bias
):
    tok_count = tokens.shape[0]
    expert_count = lax.axis_size("ep")
    capacity = min(tok_count // GROUPS, 3 * TOP_K * tok_count // (2 * expert_count))
    pair_count = tok_count * TOP_K
    flat_ids = expert_ids.reshape(pair_count)
    one_hot = (flat_ids[:, None] == jnp.arange(expert_count, dtype=jnp.int32)[None, :]).astype(
        jnp.float32
    )
    earlier = (jnp.arange(pair_count)[:, None] > jnp.arange(pair_count)[None, :]).astype(
        jnp.float32
    )
    prior_counts = jnp.dot(
        earlier, one_hot, preferred_element_type=jnp.float32, precision=lax.Precision.HIGHEST
    )
    slot_index = jnp.sum(prior_counts * one_hot, axis=1).astype(jnp.int32)
    position = flat_ids * capacity + slot_index
    owner_token = jnp.arange(pair_count, dtype=jnp.int32) // TOP_K
    slot_table = (
        jnp.full((expert_count * capacity,), tok_count, jnp.int32).at[position].set(owner_token)
    )
    gate_local = w_gate[0]
    up_local = w_up[0]
    down_local = w_down[0]
    padded = jnp.concatenate([tokens, jnp.zeros((1, tokens.shape[1]), tokens.dtype)], axis=0)
    outgoing = padded[slot_table].reshape(expert_count, capacity, tokens.shape[1])
    arrived = lax.all_to_all(outgoing, "ep", split_axis=0, concat_axis=0, tiled=True)
    sources, slot_count, slice_width = arrived.shape
    row_block = arrived.reshape(sources * slot_count, slice_width)
    row_piece = lax.all_gather(row_block, "tp", axis=1, tiled=True)
    gate_sum = jnp.dot(row_piece, gate_local, preferred_element_type=jnp.float32)
    up_sum = jnp.dot(row_piece, up_local, preferred_element_type=jnp.float32)
    hidden = (jax.nn.silu(gate_sum) * up_sum).astype(jnp.bfloat16)
    result = jnp.dot(
        lax.all_gather(hidden, "tp", axis=1, tiled=True),
        down_local,
        preferred_element_type=jnp.float32,
    )
    result = result.astype(jnp.bfloat16).reshape(sources, slot_count, down_local.shape[1])
    returned = lax.all_to_all(result, "ep", split_axis=0, concat_axis=0, tiled=True)
    flat_rows = returned.reshape(expert_count * capacity, returned.shape[2])
    picked = flat_rows[position].reshape(tok_count, TOP_K, returned.shape[2]).astype(jnp.float32)
    share_weight = (
        group_weight[:, None] * expert_weight / jnp.sum(expert_weight, axis=1, keepdims=True)
    )
    routed = jnp.einsum("tk,tkd->td", share_weight, picked)
    mixed = residual_scale * tokens.astype(jnp.float32) + routed
    first_sum, second_sum = lax.psum((jnp.sum(mixed, axis=1), jnp.sum(mixed * mixed, axis=1)), "tp")
    center = first_sum / D
    spread = second_sum / D - center * center
    centered = mixed - center[:, None]
    normed = (
        centered * lax.rsqrt(spread + norm_eps)[:, None] * norm_gain[None, :] + norm_bias[None, :]
    )
    return normed.astype(jnp.bfloat16)


MESH = pl.DeviceIdType.MESH
F32 = jnp.float32
BF16 = jnp.bfloat16
(FROM_LOWER, FROM_UPPER, ACROSS_X, ACROSS_Y, ACROSS_X2, ACROSS_Y2, RELAY_X, RELAY_Y, CORE, CORE_2,
 HIDDEN, RESULT, RESULT_2) = range(13)
KINDS = 13
BACK, SHARES, STATS = range(3)
TO_CORE, IN_PLANE, OFF_PLANE, RESULTS, HIDDENS, SHARE, STAT = range(7)


def flip(value, bits):
    bit = 1
    while bit <= bits:
        if bits & bit:
            value = value + bit - 2 * bit * lax.rem(lax.div(value, bit), 2)
        bit *= 2
    return value


def layer_kernel(
    n_plane, n_tp,
    tokens_hbm, ids_hbm, group_hbm, expert_hbm, gate_hbm, up_hbm, down_hbm, gain_hbm, bias_hbm,
    normed_out,
    tokens_ref, ids_ref, group_ref, expert_ref, gain_ref, bias_ref,
    w_in, w_out, outgoing, share_out, share_in, share_far, rows, sums, hidden, own_part, result_out,
    result_in, back_out, back_in, stats_out, stats_in,
    send_sem, recv_sem, once_sem, load_sem, entered,
):
    ep = lax.axis_index("ep")
    q = lax.axis_index("tp")
    z, x = lax.div(ep, 2), lax.rem(ep, 2)
    ox = 1 - x
    q_core, q_y, q_diag = flip(q, 1), flip(q, 2), flip(q, 3)
    core_peer, y_peer, diag_peer = (ep, q_core), (ep, q_y), (ep, q_diag)
    x_peer, corner_peer = (z * 2 + ox, q), (z * 2 + ox, flip(q, 2))

    upper = lax.rem(q, 2)
    q_up = q - upper + 1
    q_low = q_up - 1
    q_up_y = flip(q_up, 2)
    q_low_y = q_up_y - 1

    def at_plane(zz):
        return (zz * 2 + x, q)

    last = n_plane - 1
    bottom = lax.div(last - z, last)
    t1 = bottom
    t2 = n_plane // 2 - lax.div(z, 2)
    t3 = last - lax.div(z, last)
    z1 = z - 1 + 2 * bottom
    z2 = last * (1 - lax.div(z, 2))
    z3 = n_plane * last // 2 - z - z1 - z2

    tok, width = tokens_ref.shape
    cap = tok // n_plane
    half = cap // 2
    inner = gate_hbm.shape[2]

    inputs = [
        pltpu.make_async_copy(source, target, load_sem.at[3 + i])
        for i, (source, target) in enumerate((
            (ids_hbm, ids_ref), (tokens_hbm, tokens_ref), (group_hbm, group_ref),
            (expert_hbm, expert_ref), (gain_hbm, gain_ref), (bias_hbm, bias_ref),
        ))
    ]
    for load in inputs:
        load.start()

    barrier = pltpu.get_barrier_semaphore()
    for peer in (x_peer, core_peer, y_peer, diag_peer):
        pl.semaphore_signal(barrier, inc=1, device_id=peer, device_id_type=MESH)
    for zz in range(n_plane):

        @pl.when((zz > z) | (zz == z - 1))
        def _(zz=zz):
            for peer in (at_plane(zz), (zz * 2 + x, q_core)):
                pl.semaphore_signal(barrier, inc=1, device_id=peer, device_id_type=MESH)

    def tell(which, peer):
        pl.semaphore_signal(entered.at[which], inc=1, device_id=peer, device_id_type=MESH)

    loads = [
        pltpu.make_async_copy(gate_hbm.at[0], w_in.at[:, pl.ds(0, inner)], load_sem.at[0]),
        pltpu.make_async_copy(up_hbm.at[0], w_in.at[:, pl.ds(inner, inner)], load_sem.at[1]),
        pltpu.make_async_copy(down_hbm.at[0], w_out, load_sem.at[2]),
    ]
    for load in loads:
        load.start()

    @pl.when(z == last)
    def _():
        pl.semaphore_wait(barrier, n_tp + 2 * last)
        tell(1, at_plane(0))
        tell(0, at_plane(1))

    inputs[0].wait()
    first = ids_ref[0:1, :]
    group_row = (first >> 1).astype(F32)
    on_lanes = jnp.broadcast_to(group_row, (tok, tok))
    on_rows = jnp.transpose(on_lanes)
    ii = lax.broadcasted_iota(jnp.int32, (tok, tok), 0)
    jj = lax.broadcasted_iota(jnp.int32, (tok, tok), 1)
    same = on_lanes == on_rows
    zero, one = jnp.zeros((tok, tok), F32), jnp.ones((tok, tok), F32)
    rank_row = jnp.sum(jnp.where(same & (ii < jj), one, zero), axis=0, keepdims=True)
    rank_col = jnp.sum(jnp.where(same & (jj < ii), one, zero), axis=1, keepdims=True)
    place_row = group_row * cap + rank_row
    place_col = on_rows[:, 0:1] * cap + rank_col
    to_slot = jnp.broadcast_to(place_row, (tok, tok)) == ii.astype(F32)
    to_token = jnp.broadcast_to(place_col, (tok, tok)) == jj.astype(F32)

    inputs[1].wait()
    sorted_rows = jnp.dot(
        jnp.where(to_slot, one, zero).astype(BF16), tokens_ref[...], preferred_element_type=F32
    ).astype(BF16)
    outgoing[...] = sorted_rows.reshape(n_plane, cap, width)

    @pl.when(upper == 1)
    def _():
        rows[q, x, z] = outgoing[z]


    @pl.when(z < last)
    def _():
        pl.semaphore_wait(barrier, n_tp + 2 + 2 * z)

    @pl.when(z == 1)
    def _():
        tell(0, at_plane(0))

    def start(src, dst, group, arrival, peer):
        pltpu.make_async_remote_copy(
            src_ref=src, dst_ref=dst, send_sem=send_sem.at[group], recv_sem=arrival,
            device_id=peer, device_id_type=MESH,
        ).start()

    def send(block, kind, zz, peer, group=IN_PLANE):
        start(block, block, group, recv_sem.at[kind, zz], peer)

    def landed(ref, arrival):
        pltpu.make_async_copy(ref, ref, arrival).wait()

    def arrived(ref, kind, zz):
        landed(ref, recv_sem.at[kind, zz])

    low, high = pl.ds(0, half), pl.ds(half, half)

    def to_plane(zz):
        start(
            outgoing.at[zz], rows.at[q, x, z], OFF_PLANE, recv_sem.at[FROM_LOWER + upper, z],
            (zz * 2 + x, q_up),
        )

    def hand_over():
        start(outgoing.at[z], rows.at[q, x, z], TO_CORE, recv_sem.at[FROM_LOWER, z], core_peer)

    def to_core(block, zz):
        send(block, CORE, zz, core_peer, TO_CORE)

    def spread_up(zz, corner=False):
        block = rows.at[q_up, x, zz]
        if zz is not z:
            arrived(block, FROM_UPPER, zz)
        if corner:
            send(block, RELAY_Y, zz, corner_peer)
        send(block, ACROSS_X, zz, x_peer)
        send(block, ACROSS_Y2, zz, y_peer)
        to_core(block, zz)

    def spread_low(zz, corner=False):
        block = rows.at[q_low, x, zz]
        arrived(block, FROM_LOWER, zz)
        if corner:
            send(block, RELAY_X, zz, corner_peer)
        send(block, ACROSS_Y, zz, y_peer)
        send(block, ACROSS_X2, zz, x_peer)
        to_core(block, zz)

    def pass_on(zz, corner=False):
        block = rows.at[q_up, ox, zz]
        arrived(block, ACROSS_X, zz)
        if not corner:
            send(block, RELAY_Y, zz, y_peer)
        to_core(block, zz)
        block = rows.at[q_low_y, x, zz]
        arrived(block, ACROSS_Y, zz)
        if not corner:
            send(block, RELAY_X, zz, x_peer)
        to_core(block, zz)
        block = rows.at[q_low, ox, zz]
        arrived(block, ACROSS_X2, zz)
        to_core(block, zz)
        block = rows.at[q_up_y, x, zz]
        arrived(block, ACROSS_Y2, zz)
        to_core(block, zz)

    def pass_relayed(zz):
        for block, kind in (
            (rows.at[q_up_y, ox, zz], RELAY_Y), (rows.at[q_low_y, ox, zz], RELAY_X),
        ):
            arrived(block, kind, zz)
            send(block, CORE_2, zz, core_peer, TO_CORE)

    def sums_of(zz, quarter):
        part = jnp.concatenate([rows[quarter, x, zz], rows[quarter, ox, zz]], axis=0)
        w = w_in[pl.ds(pl.multiple_of(quarter * width, width), width), :]
        return jnp.dot(part, w, preferred_element_type=F32)

    def begin_hidden(zz, lower=False):
        if lower:
            arrived(rows.at[pl.ds(0, n_tp - 1), :, zz], CORE, zz)
        sums[zz] = sums_of(zz, q_low) + sums_of(zz, q_up)

    def make_hidden(zz, lower=False):
        if lower:
            arrived(rows.at[0, :, zz], CORE_2, zz)
        total = sums[zz] + (sums_of(zz, q_low_y) + sums_of(zz, q_up_y))
        gate, up = total[:, :inner], total[:, inner:]
        hidden[zz, q] = (gate / (1.0 + jnp.exp(-gate)) * up).astype(BF16)
        block = hidden.at[zz, q]
        for peer in (y_peer, diag_peer, core_peer):
            send(block, HIDDEN, zz, peer, HIDDENS)

    lane = lax.broadcasted_iota(jnp.int32, (cap, 128), 1)
    place = lax.broadcasted_iota(jnp.int32, (cap, 128), 0) + z * cap
    here = lane == place
    none = jnp.zeros((cap, 128), F32)

    def column_of(row):
        return jnp.sum(jnp.where(here, jnp.broadcast_to(row, (cap, 128)), none), axis=1, keepdims=True)

    is_first = x == 0

    def project(*blocks):
        for zz in blocks:
            arrived(hidden.at[zz, pl.ds(0, n_tp - 1)], HIDDEN, zz)
        h = jnp.concatenate(
            [
                jnp.concatenate([hidden[zz, t] for t in range(n_tp)], axis=1)
                for zz in blocks
            ],
            axis=0,
        )
        result = jnp.dot(h, w_out[...], preferred_element_type=F32).astype(BF16)
        for i, zz in enumerate(blocks):
            at = 2 * cap * i
            result_out[zz] = result[at + cap:at + 2 * cap]
            for part, kind in ((low, RESULT), (high, RESULT_2)):
                start(
                    result_out.at[zz, part], result_in.at[zz, part], RESULTS,
                    recv_sem.at[kind, zz], x_peer,
                )
        for i, zz in enumerate(blocks):
            at = 2 * cap * i
            even_share, odd_share = column_of(share_in[zz, 0:1]), column_of(share_in[zz, 1:2])
            share_own = jnp.where(is_first, even_share, odd_share)
            share_far[zz] = jnp.broadcast_to(jnp.where(is_first, odd_share, even_share), (cap, 128))
            own_part[zz] = result[at:at + cap].astype(F32) * share_own

    def give_back(zz, own=False):
        for part, at, kind in ((low, 0, RESULT), (high, half, RESULT_2)):
            arrived(result_in.at[zz, part], kind, zz)
            scaled = result_in[zz, at:at + half].astype(F32) * share_far[zz, at:at + half][:, 0:1]
            routed = (own_part[zz, at:at + half] + scaled).astype(BF16)
            if own:
                back_in[z, at:at + half] = routed
            else:
                back_out[zz, at:at + half] = routed
                start(
                    back_out.at[zz, part], back_in.at[z, part], OFF_PLANE, once_sem.at[BACK],
                    at_plane(zz),
                )
        routed = back_in[z] if own else back_out[zz]
        mixed = residual_scale * rows[q, x, zz].astype(F32) + routed.astype(F32)
        total = jnp.sum(mixed, axis=1, keepdims=True)
        centered = mixed - total / width
        square = jnp.sum(centered * centered, axis=1, keepdims=True)
        for k, column in enumerate((total, square)):
            stats_out[zz, k:k + 1] = jnp.sum(
                jnp.where(here, jnp.broadcast_to(column, (cap, 128)), none), axis=0, keepdims=True
            )
        for d in (2, 3, 1, 0):
            if own and not d:
                stats_in[z * n_tp + q] = stats_out[z]
                continue
            start(
                stats_out.at[zz], stats_in.at[z * n_tp + q], STAT, once_sem.at[STATS],
                (zz * 2 + x, flip(q, d)),
            )

    def make_shares():
        inputs[2].wait()
        inputs[3].wait()
        weights = expert_ref[...]
        share = group_ref[...] * weights / jnp.sum(weights, axis=0, keepdims=True)
        even = (first & 1) == 0
        for k in range(2):
            chosen = jnp.where(even, share[k:k + 1, :], share[1 - k:2 - k, :])
            by_token = jnp.transpose(jnp.broadcast_to(chosen, (tok, tok)))
            share_out[k:k + 1, :] = jnp.sum(jnp.where(to_token, by_token, zero), axis=0, keepdims=True)
        share_in[z] = share_out[...]
        for zz in (z1, z2, z3):
            start(share_out, share_in.at[z], SHARE, once_sem.at[SHARES], at_plane(zz))

    to_plane(t1)

    @pl.when(upper == 1)
    def _():
        spread_up(z)

    @pl.when(upper == 0)
    def _():
        hand_over()

    @pl.when(z == 0)
    def _():
        pl.semaphore_wait(entered.at[0], 1)

    to_plane(t2)

    @pl.when(z >= 2)
    def _():
        to_plane(t3)

    @pl.when(upper == 1)
    def _():
        spread_low(z)

    @pl.when(z == 0)
    def _():
        pl.semaphore_wait(entered.at[1], 1)
        to_plane(t3)


    @pl.when(upper == 1)
    def _():
        spread_up(z1)
        pass_on(z)
        spread_low(z1)
        @pl.when(z == 1)
        def _():
            pl.semaphore_wait(entered.at[0], 1)
            to_plane(t3)

        make_shares()

        @pl.when(z < 2)
        def _():
            spread_up(z2)
            spread_low(z2)

        @pl.when(z >= 2)
        def _():
            spread_up(z2, corner=True)
            spread_low(z2, corner=True)

        pass_relayed(z)
        pass_on(z1)
        spread_up(z3)
        spread_low(z3)
        loads[0].wait()
        loads[1].wait()
        begin_hidden(z)
        make_hidden(z)

        @pl.when(z >= 2)
        def _():
            pass_on(z2, corner=True)
            begin_hidden(z2)
            pass_relayed(z2)
            make_hidden(z2)

        begin_hidden(z1)
        pass_relayed(z1)
        make_hidden(z1)


        @pl.when(z >= 2)
        def _():
            pass_on(z3)
            loads[2].wait()
            landed(share_in.at[pl.ds(0, n_plane - 1)], once_sem.at[SHARES])
            project(z)
            begin_hidden(z3)

        @pl.when(z < 2)
        def _():
            pass_on(z2)
            begin_hidden(z2)
            pass_on(z3)
            loads[2].wait()
            landed(share_in.at[pl.ds(0, n_plane - 1)], once_sem.at[SHARES])
            project(z)
            begin_hidden(z3)
            pass_relayed(z2)
            make_hidden(z2)


        @pl.when(z >= 2)
        def _():
            project(z2)
            pass_relayed(z3)
            make_hidden(z3)
            project(z1)
            give_back(z2)
            project(z3)
            give_back(z, own=True)
            give_back(z1)
            give_back(z3)

        @pl.when(z < 2)
        def _():
            pass_relayed(z3)
            make_hidden(z3)
            project(z1)
            project(z2)
            give_back(z1)
            project(z3)
            give_back(z, own=True)
            give_back(z2)
            give_back(z3)

    @pl.when(upper == 0)
    def _():
        @pl.when(z == 1)
        def _():
            pl.semaphore_wait(entered.at[0], 1)
            to_plane(t3)

        make_shares()
        loads[0].wait()
        loads[1].wait()
        begin_hidden(z, lower=True)
        make_hidden(z, lower=True)

        @pl.when(z >= 2)
        def _():
            begin_hidden(z2, lower=True)
            make_hidden(z2, lower=True)
            begin_hidden(z1, lower=True)
            make_hidden(z1, lower=True)
            loads[2].wait()
            landed(share_in.at[pl.ds(0, n_plane - 1)], once_sem.at[SHARES])
            project(z)
            project(z2)
            begin_hidden(z3, lower=True)
            make_hidden(z3, lower=True)
            project(z1)
            give_back(z2)
            project(z3)
            give_back(z, own=True)
            give_back(z1)
            give_back(z3)

        @pl.when(z < 2)
        def _():
            begin_hidden(z1, lower=True)
            make_hidden(z1, lower=True)
            loads[2].wait()
            landed(share_in.at[pl.ds(0, n_plane - 1)], once_sem.at[SHARES])
            project(z)
            begin_hidden(z2, lower=True)
            make_hidden(z2, lower=True)
            begin_hidden(z3, lower=True)
            make_hidden(z3, lower=True)
            project(z1)
            project(z2)
            give_back(z1)
            project(z3)
            give_back(z, own=True)
            give_back(z2)
            give_back(z3)

    landed(back_in.at[pl.ds(0, n_plane - 1)], once_sem.at[BACK])
    routed = jnp.dot(
        jnp.where(to_token, one, zero).astype(BF16),
        back_in[...].reshape(tok, width),
        preferred_element_type=F32,
    )
    mixed = residual_scale * tokens_ref[...].astype(F32) + routed
    landed(stats_in.at[pl.ds(0, n_plane * n_tp - 1)], once_sem.at[STATS])
    pieces = [sum(stats_in[zz * n_tp + t] for zz in range(n_plane)) for t in range(n_tp)]
    full = width * n_tp
    center = sum(p[0:1] for p in pieces) / full
    spread = sum(p[1:2] + width * jnp.square(p[0:1] / width - center) for p in pieces) / full
    scale = lax.rsqrt(spread + norm_eps)
    center, scale = (
        jnp.sum(jnp.where(to_token, jnp.broadcast_to(row, (tok, tok)), zero), axis=1, keepdims=True)
        for row in (center, scale)
    )
    inputs[4].wait()
    inputs[5].wait()
    normed_out[...] = (
        (mixed - center) * scale * gain_ref[...] + bias_ref[...]
    ).astype(BF16)
    @pl.when(upper == 1)
    def _():
        landed(rows, send_sem.at[TO_CORE])
        landed(rows.at[pl.ds(0, n_tp - 1)], send_sem.at[IN_PLANE])

    @pl.when(upper == 0)
    def _():
        landed(outgoing.at[0], send_sem.at[TO_CORE])

    for group, ref in (
        (OFF_PLANE, rows.at[pl.ds(0, 2), 0, pl.ds(0, n_plane - 1)]),
        (RESULTS, result_out),
        (HIDDENS, hidden.at[:, pl.ds(0, n_tp - 1)]),
        (SHARE, share_in.at[pl.ds(0, n_plane - 1)]),
        (STAT, stats_in.at[pl.ds(0, n_plane * n_tp - 1)]),
    ):
        landed(ref, send_sem.at[group])


def pair_groups(
    tokens, expert_ids, group_weight, expert_weight, w_gate, w_up, w_down, norm_gain, norm_bias
):
    tok, width = tokens.shape
    n_plane = lax.axis_size("ep") // TOP_K
    n_tp = lax.axis_size("tp")
    cap = tok // n_plane
    inner = w_gate.shape[2]
    vmem = pl.BlockSpec(memory_space=pltpu.VMEM)
    hbm = pl.BlockSpec(memory_space=pltpu.HBM)
    return pl.pallas_call(
        functools.partial(layer_kernel, n_plane, n_tp),
        out_shape=jax.ShapeDtypeStruct((tok, width), BF16),
        in_specs=[hbm] * 9,
        out_specs=vmem,
        scratch_shapes=[
            pltpu.VMEM((tok, width), BF16),
            pltpu.VMEM((TOP_K, tok), jnp.int32),
            pltpu.VMEM((1, tok), F32),
            pltpu.VMEM((TOP_K, tok), F32),
            pltpu.VMEM((1, width), F32),
            pltpu.VMEM((1, width), F32),
            pltpu.VMEM((w_gate.shape[1], 2 * inner), BF16),
            pltpu.VMEM(w_down.shape[1:], BF16),
            pltpu.VMEM((n_plane, cap, width), BF16),
            pltpu.VMEM((2, tok), F32),
            pltpu.VMEM((n_plane, 2, tok), F32),
            pltpu.VMEM((n_plane, cap, 128), F32),
            pltpu.VMEM((n_tp, 2, n_plane, cap, width), BF16),
            pltpu.VMEM((n_plane, 2 * cap, 2 * inner), F32),
            pltpu.VMEM((n_plane, n_tp, 2 * cap, inner), BF16),
            pltpu.VMEM((n_plane, cap, width), F32),
            pltpu.VMEM((n_plane, cap, width), BF16),
            pltpu.VMEM((n_plane, cap, width), BF16),
            pltpu.VMEM((n_plane, cap, width), BF16),
            pltpu.VMEM((n_plane, cap, width), BF16),
            pltpu.VMEM((n_plane, 2, tok), F32),
            pltpu.VMEM((n_plane * n_tp, 2, tok), F32),
            pltpu.SemaphoreType.DMA((7,)),
            pltpu.SemaphoreType.DMA((KINDS, n_plane)),
            pltpu.SemaphoreType.DMA((3,)),
            pltpu.SemaphoreType.DMA((9,)),
            pltpu.SemaphoreType.REGULAR((2,)),
        ],
        compiler_params=pltpu.CompilerParams(
            collective_id=0, has_side_effects=True, vmem_limit_bytes=53 * 2**20
        ),
        name="layer",
    )(
        *(
            pltpu.with_memory_space_constraint(a, pltpu.HBM)
            for a in (
                tokens, expert_ids.T, group_weight[None, :], expert_weight.T, w_gate, w_up, w_down,
                norm_gain[None, :], norm_bias[None, :],
            )
        )
    )


def solution(mesh):
    n_ep, n_tp = mesh.shape["ep"], mesh.shape["tp"]
    pairs = TOP_K == 2 and n_ep == GROUPS * TOP_K and n_tp == 4
    return jax.shard_map(
        pair_groups if pairs else on_device,
        mesh=mesh,
        in_specs=(
            P("ep", "tp"),
            P("ep", None),
            P("ep"),
            P("ep", None),
            P("ep", None, "tp"),
            P("ep", None, "tp"),
            P("ep", None, "tp"),
            P("tp"),
            P("tp"),
        ),
        out_specs=P("ep", "tp"),
        check_vma=False,
    )
```

```python
import functools

import jax
import jax.numpy as jnp
from jax import lax
from jax.experimental import pallas as pl
from jax.experimental.pallas import tpu as pltpu
from jax.sharding import PartitionSpec as P

D = 4096
GROUPS = 4
TOP_K = 2


residual_scale = 2.0**0.5
norm_eps = 1e-05


def on_device(
    tokens, expert_ids, group_weight, expert_weight, w_gate, w_up, w_down, norm_gain, norm_bias
):
    tok_count = tokens.shape[0]
    expert_count = lax.axis_size("ep")
    capacity = min(tok_count // GROUPS, 3 * TOP_K * tok_count // (2 * expert_count))
    pair_count = tok_count * TOP_K
    flat_ids = expert_ids.reshape(pair_count)
    one_hot = (flat_ids[:, None] == jnp.arange(expert_count, dtype=jnp.int32)[None, :]).astype(
        jnp.float32
    )
    earlier = (jnp.arange(pair_count)[:, None] > jnp.arange(pair_count)[None, :]).astype(
        jnp.float32
    )
    prior_counts = jnp.dot(
        earlier, one_hot, preferred_element_type=jnp.float32, precision=lax.Precision.HIGHEST
    )
    slot_index = jnp.sum(prior_counts * one_hot, axis=1).astype(jnp.int32)
    position = flat_ids * capacity + slot_index
    owner_token = jnp.arange(pair_count, dtype=jnp.int32) // TOP_K
    slot_table = (
        jnp.full((expert_count * capacity,), tok_count, jnp.int32).at[position].set(owner_token)
    )
    gate_local = w_gate[0]
    up_local = w_up[0]
    down_local = w_down[0]
    padded = jnp.concatenate([tokens, jnp.zeros((1, tokens.shape[1]), tokens.dtype)], axis=0)
    outgoing = padded[slot_table].reshape(expert_count, capacity, tokens.shape[1])
    arrived = lax.all_to_all(outgoing, "ep", split_axis=0, concat_axis=0, tiled=True)
    sources, slot_count, slice_width = arrived.shape
    row_block = arrived.reshape(sources * slot_count, slice_width)
    row_piece = lax.all_gather(row_block, "tp", axis=1, tiled=True)
    gate_sum = jnp.dot(row_piece, gate_local, preferred_element_type=jnp.float32)
    up_sum = jnp.dot(row_piece, up_local, preferred_element_type=jnp.float32)
    hidden = (jax.nn.silu(gate_sum) * up_sum).astype(jnp.bfloat16)
    result = jnp.dot(
        lax.all_gather(hidden, "tp", axis=1, tiled=True),
        down_local,
        preferred_element_type=jnp.float32,
    )
    result = result.astype(jnp.bfloat16).reshape(sources, slot_count, down_local.shape[1])
    returned = lax.all_to_all(result, "ep", split_axis=0, concat_axis=0, tiled=True)
    flat_rows = returned.reshape(expert_count * capacity, returned.shape[2])
    picked = flat_rows[position].reshape(tok_count, TOP_K, returned.shape[2]).astype(jnp.float32)
    share_weight = (
        group_weight[:, None] * expert_weight / jnp.sum(expert_weight, axis=1, keepdims=True)
    )
    routed = jnp.einsum("tk,tkd->td", share_weight, picked)
    mixed = residual_scale * tokens.astype(jnp.float32) + routed
    first_sum, second_sum = lax.psum((jnp.sum(mixed, axis=1), jnp.sum(mixed * mixed, axis=1)), "tp")
    center = first_sum / D
    spread = second_sum / D - center * center
    centered = mixed - center[:, None]
    normed = (
        centered * lax.rsqrt(spread + norm_eps)[:, None] * norm_gain[None, :] + norm_bias[None, :]
    )
    return normed.astype(jnp.bfloat16)


MESH = pl.DeviceIdType.MESH
F32 = jnp.float32
BF16 = jnp.bfloat16
(FROM_LOWER, FROM_UPPER, ACROSS_X, ACROSS_Y, ACROSS_X2, ACROSS_Y2, RELAY_X, RELAY_Y, CORE, CORE_2,
 HIDDEN, RESULT) = range(12)
PARTS = 2
KINDS = RESULT + PARTS
BACK, SHARES, STATS = range(3)
TO_CORE, IN_PLANE, OFF_PLANE, RESULTS, HIDDENS, SHARE, STAT = range(7)


def flip(value, bits):
    bit = 1
    while bit <= bits:
        if bits & bit:
            value = value + bit - 2 * bit * lax.rem(lax.div(value, bit), 2)
        bit *= 2
    return value


def layer_kernel(
    n_plane, n_tp,
    tokens_hbm, ids_hbm, group_hbm, expert_hbm, gate_hbm, up_hbm, down_hbm, gain_hbm, bias_hbm,
    normed_out,
    tokens_ref, ids_ref, group_ref, expert_ref, gain_ref, bias_ref,
    w_in, w_out, outgoing, share_out, share_in, share_far, rows, sums, hidden, own_part, result_out,
    result_in, back_out, back_in, stats_out, stats_in,
    send_sem, recv_sem, once_sem, load_sem, entered,
):
    ep = lax.axis_index("ep")
    q = lax.axis_index("tp")
    z, x = lax.div(ep, 2), lax.rem(ep, 2)
    ox = 1 - x
    q_core, q_y, q_diag = flip(q, 1), flip(q, 2), flip(q, 3)
    core_peer, y_peer, diag_peer = (ep, q_core), (ep, q_y), (ep, q_diag)
    x_peer, corner_peer = (z * 2 + ox, q), (z * 2 + ox, flip(q, 2))

    upper = lax.rem(q, 2)
    q_up = q - upper + 1
    q_low = q_up - 1
    q_up_y = flip(q_up, 2)
    q_low_y = q_up_y - 1

    def at_plane(zz):
        return (zz * 2 + x, q)

    last = n_plane - 1
    bottom = lax.div(last - z, last)
    t1 = bottom
    t2 = n_plane // 2 - lax.div(z, 2)
    t3 = last - lax.div(z, last)
    z1 = z - 1 + 2 * bottom
    z2 = last * (1 - lax.div(z, 2))
    z3 = n_plane * last // 2 - z - z1 - z2

    tok, width = tokens_ref.shape
    cap = tok // n_plane
    step = cap // PARTS
    inner = gate_hbm.shape[2]

    inputs = [
        pltpu.make_async_copy(source, target, load_sem.at[3 + i])
        for i, (source, target) in enumerate((
            (ids_hbm, ids_ref), (tokens_hbm, tokens_ref), (group_hbm, group_ref),
            (expert_hbm, expert_ref), (gain_hbm, gain_ref), (bias_hbm, bias_ref),
        ))
    ]
    for load in inputs:
        load.start()

    barrier = pltpu.get_barrier_semaphore()
    for peer in (x_peer, core_peer, y_peer, diag_peer):
        pl.semaphore_signal(barrier, inc=1, device_id=peer, device_id_type=MESH)
    for zz in range(n_plane):

        @pl.when((zz > z) | (zz == z - 1))
        def _(zz=zz):
            for peer in (at_plane(zz), (zz * 2 + x, q_core)):
                pl.semaphore_signal(barrier, inc=1, device_id=peer, device_id_type=MESH)

    def tell(which, peer):
        pl.semaphore_signal(entered.at[which], inc=1, device_id=peer, device_id_type=MESH)

    loads = [
        pltpu.make_async_copy(gate_hbm.at[0], w_in.at[:, pl.ds(0, inner)], load_sem.at[0]),
        pltpu.make_async_copy(up_hbm.at[0], w_in.at[:, pl.ds(inner, inner)], load_sem.at[1]),
        pltpu.make_async_copy(down_hbm.at[0], w_out, load_sem.at[2]),
    ]
    for load in loads:
        load.start()

    inputs[0].wait()
    first = ids_ref[0:1, :]
    group_row = (first >> 1).astype(F32)
    on_lanes = jnp.broadcast_to(group_row, (tok, tok))
    on_rows = jnp.transpose(on_lanes)
    ii = lax.broadcasted_iota(jnp.int32, (tok, tok), 0)
    jj = lax.broadcasted_iota(jnp.int32, (tok, tok), 1)
    same = on_lanes == on_rows
    zero, one = jnp.zeros((tok, tok), F32), jnp.ones((tok, tok), F32)
    rank_row = jnp.sum(jnp.where(same & (ii < jj), one, zero), axis=0, keepdims=True)
    rank_col = jnp.sum(jnp.where(same & (jj < ii), one, zero), axis=1, keepdims=True)
    place_row = group_row * cap + rank_row
    place_col = on_rows[:, 0:1] * cap + rank_col
    to_slot = jnp.broadcast_to(place_row, (tok, tok)) == ii.astype(F32)
    to_token = jnp.broadcast_to(place_col, (tok, tok)) == jj.astype(F32)

    inputs[1].wait()
    sorted_rows = jnp.dot(
        jnp.where(to_slot, one, zero).astype(BF16), tokens_ref[...], preferred_element_type=F32
    ).astype(BF16)
    outgoing[...] = sorted_rows.reshape(n_plane, cap, width)

    @pl.when(upper == 1)
    def _():
        rows[q, x, z] = outgoing[z]


    @pl.when(z == last)
    def _():
        pl.semaphore_wait(barrier, n_tp + 2 * last)
        tell(1, at_plane(0))
        tell(0, at_plane(1))

    @pl.when(z < last)
    def _():
        pl.semaphore_wait(barrier, n_tp + 2 + 2 * z)

    @pl.when(z == 1)
    def _():
        tell(0, at_plane(0))

    def start(src, dst, group, arrival, peer):
        pltpu.make_async_remote_copy(
            src_ref=src, dst_ref=dst, send_sem=send_sem.at[group], recv_sem=arrival,
            device_id=peer, device_id_type=MESH,
        ).start()

    def send(block, kind, zz, peer, group=IN_PLANE):
        start(block, block, group, recv_sem.at[kind, zz], peer)

    def landed(ref, arrival):
        pltpu.make_async_copy(ref, ref, arrival).wait()

    def arrived(ref, kind, zz):
        landed(ref, recv_sem.at[kind, zz])

    def to_plane(zz):
        start(
            outgoing.at[zz], rows.at[q, x, z], OFF_PLANE, recv_sem.at[FROM_LOWER + upper, z],
            (zz * 2 + x, q_up),
        )

    def hand_over():
        start(outgoing.at[z], rows.at[q, x, z], TO_CORE, recv_sem.at[FROM_LOWER, z], core_peer)

    def to_core(block, zz):
        send(block, CORE, zz, core_peer, TO_CORE)

    def spread_up(zz, corner=False):
        block = rows.at[q_up, x, zz]
        if zz is not z:
            arrived(block, FROM_UPPER, zz)
        if corner:
            send(block, RELAY_Y, zz, corner_peer)
        send(block, ACROSS_X, zz, x_peer)
        send(block, ACROSS_Y2, zz, y_peer)
        to_core(block, zz)

    def spread_low(zz, corner=False):
        block = rows.at[q_low, x, zz]
        arrived(block, FROM_LOWER, zz)
        if corner:
            send(block, RELAY_X, zz, corner_peer)
        send(block, ACROSS_Y, zz, y_peer)
        send(block, ACROSS_X2, zz, x_peer)
        to_core(block, zz)

    def pass_on(zz, corner=False):
        block = rows.at[q_up, ox, zz]
        arrived(block, ACROSS_X, zz)
        if not corner:
            send(block, RELAY_Y, zz, y_peer)
        to_core(block, zz)
        block = rows.at[q_low_y, x, zz]
        arrived(block, ACROSS_Y, zz)
        if not corner:
            send(block, RELAY_X, zz, x_peer)
        to_core(block, zz)
        block = rows.at[q_low, ox, zz]
        arrived(block, ACROSS_X2, zz)
        to_core(block, zz)
        block = rows.at[q_up_y, x, zz]
        arrived(block, ACROSS_Y2, zz)
        to_core(block, zz)

    def pass_relayed(zz):
        for block, kind in (
            (rows.at[q_up_y, ox, zz], RELAY_Y), (rows.at[q_low_y, ox, zz], RELAY_X),
        ):
            arrived(block, kind, zz)
            send(block, CORE_2, zz, core_peer, TO_CORE)

    def sums_of(zz, quarter):
        part = jnp.concatenate([rows[quarter, x, zz], rows[quarter, ox, zz]], axis=0)
        w = w_in[pl.ds(pl.multiple_of(quarter * width, width), width), :]
        return jnp.dot(part, w, preferred_element_type=F32)

    def begin_hidden(zz, lower=False):
        if lower:
            arrived(rows.at[pl.ds(0, n_tp - 1), :, zz], CORE, zz)
        sums[zz] = sums_of(zz, q_low) + sums_of(zz, q_up)

    def make_hidden(zz, lower=False):
        if lower:
            arrived(rows.at[0, :, zz], CORE_2, zz)
        total = sums[zz] + (sums_of(zz, q_low_y) + sums_of(zz, q_up_y))
        gate, up = total[:, :inner], total[:, inner:]
        hidden[zz, q] = (gate / (1.0 + jnp.exp(-gate)) * up).astype(BF16)
        block = hidden.at[zz, q]
        for peer in (y_peer, diag_peer, core_peer):
            send(block, HIDDEN, zz, peer, HIDDENS)

    lane = lax.broadcasted_iota(jnp.int32, (cap, 128), 1)
    place = lax.broadcasted_iota(jnp.int32, (cap, 128), 0) + z * cap
    here = lane == place
    none = jnp.zeros((cap, 128), F32)

    def column_of(row):
        return jnp.sum(jnp.where(here, jnp.broadcast_to(row, (cap, 128)), none), axis=1, keepdims=True)

    is_first = x == 0

    def project(*blocks):
        for zz in blocks:
            arrived(hidden.at[zz, pl.ds(0, n_tp - 1)], HIDDEN, zz)
        h = jnp.concatenate(
            [
                jnp.concatenate([hidden[zz, t] for t in range(n_tp)], axis=1)
                for zz in blocks
            ],
            axis=0,
        )
        result = jnp.dot(h, w_out[...], preferred_element_type=F32).astype(BF16)
        for i, zz in enumerate(blocks):
            at = 2 * cap * i
            result_out[zz] = result[at + cap:at + 2 * cap]
            for n in range(PARTS):
                part, kind = pl.ds(n * step, step), RESULT + n
                start(
                    result_out.at[zz, part], result_in.at[zz, part], RESULTS,
                    recv_sem.at[kind, zz], x_peer,
                )
        for i, zz in enumerate(blocks):
            at = 2 * cap * i
            even_share, odd_share = column_of(share_in[zz, 0:1]), column_of(share_in[zz, 1:2])
            share_own = jnp.where(is_first, even_share, odd_share)
            share_far[zz] = jnp.broadcast_to(jnp.where(is_first, odd_share, even_share), (cap, 128))
            own_part[zz] = result[at:at + cap].astype(F32) * share_own

    def give_back(zz, own=False):
        for i in range(PARTS):
            at, part, kind = i * step, pl.ds(i * step, step), RESULT + i
            arrived(result_in.at[zz, part], kind, zz)
            scaled = result_in[zz, at:at + step].astype(F32) * share_far[zz, at:at + step][:, 0:1]
            routed = (own_part[zz, at:at + step] + scaled).astype(BF16)
            if own:
                back_in[z, at:at + step] = routed
            else:
                back_out[zz, at:at + step] = routed
                start(
                    back_out.at[zz, part], back_in.at[z, part], OFF_PLANE, once_sem.at[BACK],
                    at_plane(zz),
                )
        routed = back_in[z] if own else back_out[zz]
        mixed = residual_scale * rows[q, x, zz].astype(F32) + routed.astype(F32)
        total = jnp.sum(mixed, axis=1, keepdims=True)
        centered = mixed - total / width
        square = jnp.sum(centered * centered, axis=1, keepdims=True)
        for k, column in enumerate((total, square)):
            stats_out[zz, k:k + 1] = jnp.sum(
                jnp.where(here, jnp.broadcast_to(column, (cap, 128)), none), axis=0, keepdims=True
            )
        for d in (2, 3, 1, 0):
            if own and not d:
                stats_in[z * n_tp + q] = stats_out[z]
                continue
            start(
                stats_out.at[zz], stats_in.at[z * n_tp + q], STAT, once_sem.at[STATS],
                (zz * 2 + x, flip(q, d)),
            )

    def make_shares():
        inputs[2].wait()
        inputs[3].wait()
        weights = expert_ref[...]
        share = group_ref[...] * weights / jnp.sum(weights, axis=0, keepdims=True)
        even = (first & 1) == 0
        for k in range(2):
            chosen = jnp.where(even, share[k:k + 1, :], share[1 - k:2 - k, :])
            by_token = jnp.transpose(jnp.broadcast_to(chosen, (tok, tok)))
            share_out[k:k + 1, :] = jnp.sum(jnp.where(to_token, by_token, zero), axis=0, keepdims=True)
        share_in[z] = share_out[...]
        for zz in (z1, z2, z3):
            start(share_out, share_in.at[z], SHARE, once_sem.at[SHARES], at_plane(zz))

    to_plane(t1)

    @pl.when(upper == 1)
    def _():
        spread_up(z)

    @pl.when(upper == 0)
    def _():
        hand_over()

    @pl.when(z == 0)
    def _():
        pl.semaphore_wait(entered.at[0], 1)

    to_plane(t2)

    @pl.when(z >= 2)
    def _():
        to_plane(t3)

    @pl.when(upper == 1)
    def _():
        spread_low(z)

    @pl.when(z == 0)
    def _():
        pl.semaphore_wait(entered.at[1], 1)
        to_plane(t3)


    @pl.when(upper == 1)
    def _():
        spread_up(z1)
        pass_on(z)
        spread_low(z1)
        @pl.when(z == 1)
        def _():
            pl.semaphore_wait(entered.at[0], 1)
            to_plane(t3)

        make_shares()

        @pl.when(z < 2)
        def _():
            spread_up(z2)
            spread_low(z2)

        @pl.when(z >= 2)
        def _():
            spread_up(z2, corner=True)
            spread_low(z2, corner=True)

        pass_relayed(z)
        pass_on(z1)
        spread_up(z3)
        spread_low(z3)
        loads[0].wait()
        loads[1].wait()
        begin_hidden(z)
        make_hidden(z)

        @pl.when(z >= 2)
        def _():
            pass_on(z2, corner=True)
            begin_hidden(z2)
            pass_relayed(z2)
            make_hidden(z2)
            begin_hidden(z1)
            pass_relayed(z1)
            make_hidden(z1)
            pass_on(z3)
            loads[2].wait()
            landed(share_in.at[pl.ds(0, n_plane - 1)], once_sem.at[SHARES])
            project(z)
            begin_hidden(z3)
            pass_relayed(z3)
            project(z2)
            make_hidden(z3)
            project(z1)
            give_back(z2)
            project(z3)
            give_back(z, own=True)
            give_back(z1)
            give_back(z3)

        @pl.when(z < 2)
        def _():
            begin_hidden(z1)
            pass_relayed(z1)
            make_hidden(z1)
            pass_on(z2)
            begin_hidden(z2)
            pass_on(z3)
            loads[2].wait()
            landed(share_in.at[pl.ds(0, n_plane - 1)], once_sem.at[SHARES])
            project(z)
            begin_hidden(z3)
            pass_relayed(z2)
            make_hidden(z2)
            pass_relayed(z3)
            make_hidden(z3)
            project(z1)
            project(z2)
            give_back(z1)
            project(z3)
            give_back(z, own=True)
            give_back(z2)
            give_back(z3)

    @pl.when(upper == 0)
    def _():
        @pl.when(z == 1)
        def _():
            pl.semaphore_wait(entered.at[0], 1)
            to_plane(t3)

        make_shares()
        loads[0].wait()
        loads[1].wait()
        begin_hidden(z, lower=True)
        make_hidden(z, lower=True)

        @pl.when(z >= 2)
        def _():
            begin_hidden(z2, lower=True)
            make_hidden(z2, lower=True)
            begin_hidden(z1, lower=True)
            make_hidden(z1, lower=True)
            loads[2].wait()
            landed(share_in.at[pl.ds(0, n_plane - 1)], once_sem.at[SHARES])
            project(z)
            project(z2)
            begin_hidden(z3, lower=True)
            make_hidden(z3, lower=True)
            project(z1)
            give_back(z2)
            project(z3)
            give_back(z, own=True)
            give_back(z1)
            give_back(z3)

        @pl.when(z < 2)
        def _():
            begin_hidden(z1, lower=True)
            make_hidden(z1, lower=True)
            loads[2].wait()
            landed(share_in.at[pl.ds(0, n_plane - 1)], once_sem.at[SHARES])
            project(z)
            begin_hidden(z2, lower=True)
            make_hidden(z2, lower=True)
            begin_hidden(z3, lower=True)
            make_hidden(z3, lower=True)
            project(z1)
            project(z2)
            give_back(z1)
            project(z3)
            give_back(z, own=True)
            give_back(z2)
            give_back(z3)

    landed(back_in.at[pl.ds(0, n_plane - 1)], once_sem.at[BACK])
    routed = jnp.dot(
        jnp.where(to_token, one, zero).astype(BF16),
        back_in[...].reshape(tok, width),
        preferred_element_type=F32,
    )
    mixed = residual_scale * tokens_ref[...].astype(F32) + routed
    landed(stats_in.at[pl.ds(0, n_plane * n_tp - 1)], once_sem.at[STATS])
    pieces = [sum(stats_in[zz * n_tp + t] for zz in range(n_plane)) for t in range(n_tp)]
    full = width * n_tp
    center = sum(p[0:1] for p in pieces) / full
    spread = sum(p[1:2] + width * jnp.square(p[0:1] / width - center) for p in pieces) / full
    scale = lax.rsqrt(spread + norm_eps)
    center, scale = (
        jnp.sum(jnp.where(to_token, jnp.broadcast_to(row, (tok, tok)), zero), axis=1, keepdims=True)
        for row in (center, scale)
    )
    inputs[4].wait()
    inputs[5].wait()
    normed_out[...] = (
        (mixed - center) * scale * gain_ref[...] + bias_ref[...]
    ).astype(BF16)
    @pl.when(upper == 1)
    def _():
        landed(rows, send_sem.at[TO_CORE])
        landed(rows.at[pl.ds(0, n_tp - 1)], send_sem.at[IN_PLANE])

    @pl.when(upper == 0)
    def _():
        landed(outgoing.at[0], send_sem.at[TO_CORE])

    for group, ref in (
        (OFF_PLANE, rows.at[pl.ds(0, 2), 0, pl.ds(0, n_plane - 1)]),
        (RESULTS, result_out),
        (HIDDENS, hidden.at[:, pl.ds(0, n_tp - 1)]),
        (SHARE, share_in.at[pl.ds(0, n_plane - 1)]),
        (STAT, stats_in.at[pl.ds(0, n_plane * n_tp - 1)]),
    ):
        landed(ref, send_sem.at[group])


def pair_groups(
    tokens, expert_ids, group_weight, expert_weight, w_gate, w_up, w_down, norm_gain, norm_bias
):
    tok, width = tokens.shape
    n_plane = lax.axis_size("ep") // TOP_K
    n_tp = lax.axis_size("tp")
    cap = tok // n_plane
    inner = w_gate.shape[2]
    vmem = pl.BlockSpec(memory_space=pltpu.VMEM)
    hbm = pl.BlockSpec(memory_space=pltpu.HBM)
    return pl.pallas_call(
        functools.partial(layer_kernel, n_plane, n_tp),
        out_shape=jax.ShapeDtypeStruct((tok, width), BF16),
        in_specs=[hbm] * 9,
        out_specs=vmem,
        scratch_shapes=[
            pltpu.VMEM((tok, width), BF16),
            pltpu.VMEM((TOP_K, tok), jnp.int32),
            pltpu.VMEM((1, tok), F32),
            pltpu.VMEM((TOP_K, tok), F32),
            pltpu.VMEM((1, width), F32),
            pltpu.VMEM((1, width), F32),
            pltpu.VMEM((w_gate.shape[1], 2 * inner), BF16),
            pltpu.VMEM(w_down.shape[1:], BF16),
            pltpu.VMEM((n_plane, cap, width), BF16),
            pltpu.VMEM((2, tok), F32),
            pltpu.VMEM((n_plane, 2, tok), F32),
            pltpu.VMEM((n_plane, cap, 128), F32),
            pltpu.VMEM((n_tp, 2, n_plane, cap, width), BF16),
            pltpu.VMEM((n_plane, 2 * cap, 2 * inner), F32),
            pltpu.VMEM((n_plane, n_tp, 2 * cap, inner), BF16),
            pltpu.VMEM((n_plane, cap, width), F32),
            pltpu.VMEM((n_plane, cap, width), BF16),
            pltpu.VMEM((n_plane, cap, width), BF16),
            pltpu.VMEM((n_plane, cap, width), BF16),
            pltpu.VMEM((n_plane, cap, width), BF16),
            pltpu.VMEM((n_plane, 2, tok), F32),
            pltpu.VMEM((n_plane * n_tp, 2, tok), F32),
            pltpu.SemaphoreType.DMA((7,)),
            pltpu.SemaphoreType.DMA((KINDS, n_plane)),
            pltpu.SemaphoreType.DMA((3,)),
            pltpu.SemaphoreType.DMA((9,)),
            pltpu.SemaphoreType.REGULAR((2,)),
        ],
        compiler_params=pltpu.CompilerParams(
            collective_id=0, has_side_effects=True, vmem_limit_bytes=53 * 2**20
        ),
        name="layer",
    )(
        *(
            pltpu.with_memory_space_constraint(a, pltpu.HBM)
            for a in (
                tokens, expert_ids.T, group_weight[None, :], expert_weight.T, w_gate, w_up, w_down,
                norm_gain[None, :], norm_bias[None, :],
            )
        )
    )


def solution(mesh):
    n_ep, n_tp = mesh.shape["ep"], mesh.shape["tp"]
    pairs = TOP_K == 2 and n_ep == GROUPS * TOP_K and n_tp == 4
    return jax.shard_map(
        pair_groups if pairs else on_device,
        mesh=mesh,
        in_specs=(
            P("ep", "tp"),
            P("ep", None),
            P("ep"),
            P("ep", None),
            P("ep", None, "tp"),
            P("ep", None, "tp"),
            P("ep", None, "tp"),
            P("tp"),
            P("tp"),
        ),
        out_specs=P("ep", "tp"),
        check_vma=False,
    )
```
